32 devices in a mesh: sp: 8 (over z, x), dp: 4 (over y, core).
Axes of the slice: x: 2, y: 2, z: 4, core: 2. Of those that a mesh axis runs over, the one named last changes fastest.
Arguments:
- tokens: bfloat16 [4, 4096, 4096], P('dp', 'sp'), may hold values from -6 to 6
- documents: int32 [4, 4096], P('dp', 'sp'), may hold values from 0 to 7, never falling along the last dimension, each value on 1 to 1024 neighbouring positions
- value_weight: bfloat16 [4096, 2048], P(('sp', 'dp')), may hold values from -0.09375 to 0.09375
- gate_weight: bfloat16 [4096, 2048], P(('sp', 'dp')), may hold values from -0.09375 to 0.09375
- conv_weight: bfloat16 [31, 2048], replicated, may hold values from -1 to 1
- norm_gain: float32 [2048], replicated, may hold values from 0.1 to 1.9
- norm_bias: float32 [2048], replicated, may hold values from -2 to 2
Outputs:
- activated: bfloat16 [4, 4096, 2048], P('dp', 'sp')
The draws below stay inside these ranges and needn't reach their ends.
Inputs may be any that keep to these rules, and one draw needn't show every extreme that they name: `documents`: document numbers never fall along a sequence, run from 0 to 7, and each document covers 1 to 1024 positions.
All inputs are finite; a program needn't handle non-finite values.
Results may differ from the reference program's by a relative error of at most 0.0064.
Values may be sent and summed in bfloat16 or wider, within the bound.
A program may use at most 192 MiB of HBM per device.

```python
import math
import jax
import jax.numpy as jnp
import numpy as np
from jax import lax

D = 4096
DB = 2048
KERNEL = 31
DOCS = 8
LENGTH = 4096
BATCH = 4


def levels(key, extent, pieces, smallest, high):
    def one(position, blocks):
        heights = jax.random.uniform(jax.random.fold_in(jax.random.fold_in(key, 6), position), (blocks,), jnp.float32, smallest / len(pieces), high / len(pieces))
        return jnp.repeat(jnp.exp(heights), extent[position] // blocks).reshape((-1,) + (1,) * (len(extent) - position - 1))

    factor_of = one(*pieces[0])
    for cut in pieces[1:]:
        factor_of = factor_of * one(*cut)
    return factor_of


def length_profile(amount, total, most, lean):
    portions = [(1 << 20) // math.isqrt(standing ** lean) + 1 for standing in range(2, amount + 1)]
    surplus, given = total - most - (amount - 1), [1] * (amount - 1)
    while surplus > 0:
        candidates = [i for i in range(amount - 1) if given[i] < most]
        pool, budget = sum([portions[i] for i in candidates]), surplus
        for i in candidates:
            extra = min(most - given[i], max(1, budget * portions[i] // pool), surplus)
            given[i] = given[i] + extra
            surplus = surplus - extra
    return np.array([most] + given)


def uneven(stream_key, number_of, total, reach, lean):
    if number_of == 2:
        one = jax.random.randint(stream_key, (), max(1, total - reach), min(reach, total - 1) + 1)
        return jnp.stack([one, total - one])
    tallies = jnp.asarray(length_profile(number_of, total, reach, lean), jnp.int32)
    twos = (number_of - 1) // 2
    donor, sink = tallies[1:1 + 2 * twos:2], tallies[2:2 + 2 * twos:2]
    slack = jnp.minimum(donor - 1, reach - sink)
    shifted = jax.random.randint(jax.random.fold_in(stream_key, 1), (twos,), 0, 1 << 20) % (slack + 1)
    tallies = tallies.at[1:1 + 2 * twos:2].set(donor - shifted).at[2:2 + 2 * twos:2].set(sink + shifted)
    return tallies[jax.random.permutation(jax.random.fold_in(stream_key, 2), number_of)]


def bell_draw(stream_key, dims, scale, bound, cuts=(), dtype=jnp.bfloat16):
    factor_of = levels(stream_key, dims, cuts, -0.22, 0.18) if cuts else 1.0
    entries = jax.random.normal(stream_key, dims, jnp.float32) * scale * factor_of
    return jnp.minimum(jnp.maximum(entries, -bound), bound).astype(dtype)


def setup_inputs(seed: int = 0) -> dict:
    streams_of = jax.random.split(jax.random.key(seed), 8)
    tokens = bell_draw(streams_of[0], (BATCH, LENGTH, D), 1.0, 6.0, ((0, 4), (1, 8)))
    documents = jax.vmap(lambda own: jnp.searchsorted(jnp.cumsum(uneven(own, DOCS, LENGTH, LENGTH // 4, 1)), jnp.arange(LENGTH), side="right"))(jax.random.split(streams_of[1], BATCH)).reshape((BATCH, LENGTH)).astype(jnp.int32)
    value_weight = bell_draw(streams_of[2], (D, DB), D ** -0.5, 0.09375, ((0, 32),))
    gate_weight = bell_draw(streams_of[3], (D, DB), D ** -0.5, 0.09375, ((0, 32),))
    conv_weight = bell_draw(streams_of[4], (KERNEL, DB), KERNEL ** -0.5, 1.0)
    norm_gain = jnp.clip(1.0 + 0.18 * jax.random.normal(streams_of[5], (DB,), jnp.float32), 0.1, 1.9)
    norm_bias = bell_draw(streams_of[6], (DB,), 0.5, 2.0, (), jnp.float32)
    return dict(tokens=tokens, documents=documents, value_weight=value_weight, gate_weight=gate_weight, conv_weight=conv_weight, norm_gain=norm_gain, norm_bias=norm_bias)


def convolve(padded, padded_docs, taps, count):
    lead = taps.shape[0] - 1
    here = padded_docs[:, lead:lead + count]
    total = jnp.zeros((padded.shape[0], count, padded.shape[2]), jnp.float32)
    for lag in range(taps.shape[0]):
        begin = lead - lag
        moved = padded[:, begin:begin + count].astype(jnp.float32)
        keep = (padded_docs[:, begin:begin + count] == here)[:, :, None]
        total = total + jnp.where(keep, moved, 0.0) * taps[lag].astype(jnp.float32)
    return total

def finish(mixed, norm_gain, norm_bias):
    wide = mixed.astype(jnp.float32)
    center = wide - lax.optimization_barrier(jnp.mean(wide, axis=-1, keepdims=True))
    spread = lax.optimization_barrier(jnp.mean(center * center, axis=-1, keepdims=True))
    normed = center * lax.rsqrt(spread + 1e-06) * norm_gain + norm_bias
    return jax.nn.silu(normed).astype(jnp.bfloat16)

def reference(tokens, documents, value_weight, gate_weight, conv_weight, norm_gain, norm_bias):
    lead = KERNEL - 1

    def one_row(pair):
        rows, row_docs = pair
        value = jnp.dot(rows, value_weight, preferred_element_type=jnp.float32).astype(jnp.bfloat16)
        gate = jnp.dot(rows, gate_weight, preferred_element_type=jnp.float32).astype(jnp.bfloat16)
        value, gate = lax.optimization_barrier((value, gate))
        glu = (value.astype(jnp.float32) * jax.nn.sigmoid(gate.astype(jnp.float32))).astype(jnp.bfloat16)
        glu = lax.optimization_barrier(glu)
        padded = jnp.pad(glu[None], ((0, 0), (lead, 0), (0, 0)))
        padded_docs = jnp.pad(row_docs[None], ((0, 0), (lead, 0)), constant_values=-1)
        mixed = convolve(padded, padded_docs, conv_weight, rows.shape[0]).astype(jnp.bfloat16)
        mixed = lax.optimization_barrier(mixed)
        return finish(mixed, norm_gain, norm_bias)[0]
    return lax.map(one_row, (tokens, documents))
```

```python
import functools

import jax
import jax.numpy as jnp
from jax import lax
from jax.experimental import pallas as pl
from jax.experimental.pallas import tpu as pltpu
from jax.sharding import PartitionSpec as P

KERNEL = 31
HALO = 32
LANES = 128
TILE = 64
AHEAD = 1
KEPT = 5
MESH = pl.DeviceIdType.MESH


def fused_kernel(
    side, tall, blocks, tok_hbm, docs_hbm, value_hbm, gate_hbm, conv_ref, mixed_ref,
    weights, tok, docs, taps, shifted, far, near_by, send, recv, cross, own, begin, halo
):
    sp, dp = lax.axis_index("sp"), lax.axis_index("dp")
    sp_size = lax.axis_size("sp")
    core, y = lax.rem(dp, 2), lax.div(dp, 2)
    z, x = lax.div(sp, side), lax.rem(sp, side)
    flip = core == 1
    u, v = jnp.where(flip, y, x), jnp.where(flip, x, y)
    depth = value_hbm.shape[0]
    count = tok_hbm.shape[0]
    parts = tall // 2
    second_start, third_start = 2, 6
    late_start = third_start + tall
    other = {"sp": sp, "dp": y * 2 + (1 - core)}
    here = (z * side + x) * side + y

    def device(dz, du, dv):
        dx, dy = jnp.where(flip, dv, du), jnp.where(flip, du, dv)
        return {"sp": dz * side + dx, "dp": dy * 2 + core}

    def number(pz, pu, pv):
        px, py = jnp.where(flip, pv, pu), jnp.where(flip, pu, pv)
        return (pz * side + px) * side + py

    def piece(which, block, q):
        return weights.at[
            block, pl.ds(pl.multiple_of((q * 2 + which) * depth, depth), depth), :
        ]

    def link(kind, block, q, target):
        return pltpu.make_async_remote_copy(
            src_ref=piece(core, block, q),
            dst_ref=piece(core, block, q),
            send_sem=send.at[kind, lax.rem(block, KEPT), q],
            recv_sem=recv.at[block, q],
            device_id=target,
            device_id_type=MESH,
        )

    def hand_over(which, block, q):
        return pltpu.make_async_remote_copy(
            src_ref=piece(which, block, q),
            dst_ref=piece(which, block, q),
            send_sem=send.at[6, lax.rem(block, KEPT), q],
            recv_sem=cross.at[block, q],
            device_id=other,
            device_id_type=MESH,
        )

    def routes(block, pz, pu, pv, act):
        q = number(pz, pu, pv)
        tall_first = (block == 1) | (block == 4) | (block == 6)
        home_u, home_v, home_z = u == pu, v == pv, z == pz
        along_z = home_v & (home_u | jnp.logical_not(tall_first))
        along_u = home_v & (home_z | tall_first)
        ways = (
            (along_z & (z >= pz) & (z + 1 < tall), (z + 1, u, v)),
            (along_z & (z <= pz) & (z > 0), (z - 1, u, v)),
            (along_u & (u >= pu) & (u + 1 < side), (z, u + 1, v)),
            (along_u & (u <= pu) & (u > 0), (z, u - 1, v)),
            ((v >= pv) & (v + 1 < side), (z, u, v + 1)),
            ((v <= pv) & (v > 0), (z, u, v - 1)),
        )
        for kind, (taken, target) in enumerate(ways):

            @pl.when(taken)
            def _(kind=kind, target=target):
                act(link(kind, block, q, device(*target)))

        act(hand_over(core, block, q))

    def pass_on(block, pz, pu, pv):
        routes(block, pz, pu, pv, lambda copy: copy.start())

    def arrived(block, pz, pu, pv):
        link(0, block, number(pz, pu, pv), other).wait_recv()
        pass_on(block, pz, pu, pv)

    low = jnp.minimum(z, tall - 1 - z)

    def near(k):
        step = jnp.where(lax.rem(k, 2) == 1, low - lax.div(k + 1, 2), low + lax.div(k, 2))
        at = jnp.where(k <= 2 * low, step, k)
        return jnp.where(z == low, at, tall - 1 - at)

    def own_copies(block):
        rows = pl.ds(pl.multiple_of((here * 2 + core) * depth, depth), depth)
        for part in range(parts):
            first = pl.multiple_of((block * parts + part) * LANES, LANES)
            for half, source in enumerate((value_hbm, gate_hbm)):
                yield pltpu.make_async_copy(
                    source.at[:, pl.ds(first, LANES)],
                    weights.at[block, rows, pl.ds((2 * part + half) * LANES, LANES)],
                    own.at[block, 2 * part + half],
                )

    def send_own(block):
        for copy in own_copies(block):
            copy.wait()
        pass_on(block, z, u, v)

    @pl.loop(0, blocks)
    def _(block):
        for copy in own_copies(block):
            copy.start()

    load = pltpu.make_async_copy(tok_hbm, tok.at[pl.ds(HALO, count), :], begin.at[0])
    load.start()
    read = pltpu.make_async_copy(docs_hbm, docs.at[:, pl.ds(LANES, count)], begin.at[1])
    read.start()

    barrier = pltpu.get_barrier_semaphore()
    greeted = jnp.int32(1)
    pl.semaphore_signal(barrier, inc=1, device_id=other, device_id_type=MESH)
    for there, target in (
        (z + 1 < tall, device(z + 1, u, v)),
        (z > 0, device(z - 1, u, v)),
        (u + 1 < side, device(z, u + 1, v)),
        (u > 0, device(z, u - 1, v)),
        (v + 1 < side, device(z, u, v + 1)),
        (v > 0, device(z, u, v - 1)),
        (sp + 1 < sp_size, {"sp": sp + 1, "dp": dp}),
        (sp > 0, {"sp": sp - 1, "dp": dp}),
    ):
        greeted = greeted + there.astype(jnp.int32)

        @pl.when(there)
        def _(target=target):
            pl.semaphore_signal(barrier, inc=1, device_id=target, device_id_type=MESH)

    pl.semaphore_wait(barrier, greeted)

    following = {"sp": lax.rem(sp + 1, sp_size), "dp": dp}
    tail = pltpu.make_async_remote_copy(
        src_ref=tok_hbm.at[pl.ds(count - HALO, HALO), :],
        dst_ref=tok.at[pl.ds(0, HALO), :],
        send_sem=halo.at[0],
        recv_sem=halo.at[1],
        device_id=following,
        device_id_type=MESH,
    )
    docs_tail = pltpu.make_async_remote_copy(
        src_ref=docs_hbm.at[:, pl.ds(count - LANES, LANES)],
        dst_ref=docs.at[:, pl.ds(0, LANES)],
        send_sem=halo.at[2],
        recv_sem=halo.at[3],
        device_id=following,
        device_id_type=MESH,
    )

    @pl.loop(0, AHEAD)
    def _(block):
        send_own(block)

    @pl.when(sp + 1 < sp_size)
    def _():
        tail.start()
        docs_tail.start()

    @pl.when(sp == 0)
    def _():
        tok[pl.ds(0, HALO), :] = jnp.zeros((HALO, tok.shape[1]), tok.dtype)
        docs[:, pl.ds(0, LANES)] = jnp.full((1, LANES), -1, jnp.int32)

    taps[pl.ds(0, KERNEL), :] = conv_ref[...].astype(jnp.float32)

    def prepare():
        load.wait()
        read.wait()

        @pl.when(sp > 0)
        def _():
            tail.wait_recv()
            docs_tail.wait_recv()

        column = jnp.broadcast_to(docs[...], (LANES, LANES + count)).T
        spread = column[LANES - HALO :]
        for lag in range(8, HALO, 8):
            same = spread[HALO - 8 :] == spread[HALO - 8 - lag : HALO + count - lag]
            far[lag // 8 - 1, pl.ds(HALO - 8, count + 8), :] = same.astype(jnp.float32)
        for lag in range(1, 8):
            same = spread[HALO:] == spread[HALO - lag : HALO + count - lag]
            near_by[lag - 1] = same.astype(jnp.float32)

    def project(block, part):
        held = weights[
            block, :, pl.ds(pl.multiple_of(part * 2 * LANES, 2 * LANES), 2 * LANES)
        ]
        both = jnp.dot(tok[...], held, preferred_element_type=jnp.float32)
        value = both[:, :LANES].astype(jnp.bfloat16).astype(jnp.float32)
        gate = both[:, LANES:].astype(jnp.bfloat16).astype(jnp.float32)
        glu = (value * jax.nn.sigmoid(gate)).astype(jnp.bfloat16).astype(jnp.float32)
        shifted[0] = glu

    def convolve(block, part):
        first = pl.multiple_of((block * parts + part) * LANES, LANES)
        lanes = pl.ds(first, LANES)
        kept = pl.ds(HALO - 8, count + 8)
        for a in range(1, HALO // 8):
            shifted[a, kept, :] = (
                shifted[0, pl.ds(HALO - 8 - 8 * a, count + 8), :] * far[a - 1, kept, :]
            )

        @pl.loop(0, count // TILE)
        def _(tile):
            top = pl.multiple_of(tile * TILE, TILE)
            total = None
            for r in range(8):
                run = None
                for a in range(HALO // 8):
                    lag = 8 * a + r
                    if lag < KERNEL:
                        moved = shifted[a, pl.ds(top + HALO - r, TILE), :]
                        term = moved * taps[lag : lag + 1, lanes]
                        run = term if run is None else run + term
                if r:
                    run = run * near_by[r - 1, pl.ds(top, TILE), :]
                total = run if total is None else total + run
            mixed_ref[pl.ds(top, TILE), lanes] = total.astype(jnp.bfloat16)

    def tick(at, carry):
        block, k = lax.div(at, tall), lax.rem(at, tall)

        @pl.when((block + AHEAD < blocks) & (k == 0))
        def _():
            send_own(block + AHEAD)

        @pl.when((block < blocks) & (k > 0))
        def _():
            arrived(block, near(k), u, v)

        second = jnp.maximum(at - second_start, 0)
        block2, k2 = lax.div(second, tall), lax.rem(second, tall)

        @pl.when((at >= second_start) & (block2 < blocks))
        def _():
            @pl.loop(1, side)
            def _(du):
                arrived(block2, near(k2), lax.rem(u + du, side), v)

        third = jnp.maximum(at - third_start, 0)
        block3, k3 = lax.div(third, tall), lax.rem(third, tall)

        @pl.when((at >= third_start) & (block3 < blocks))
        def _():
            @pl.loop(0, side)
            def _(du):
                @pl.loop(1, side)
                def _(dv):
                    arrived(block3, near(k3), lax.rem(u + du, side), lax.rem(v + dv, side))

        late = jnp.maximum(at - late_start, 0)
        block4, k4 = lax.div(late, tall), lax.rem(late, tall)

        @pl.when(at == second_start)
        def _():
            prepare()

        @pl.when((at >= late_start) & (k4 == 0))
        def _():
            @pl.loop(0, tall * side * side)
            def _(q):
                hand_over(1 - core, block4, q).wait_recv()

        part = lax.div(k4, 2)

        @pl.when((at >= late_start) & (lax.rem(k4, 2) == 0))
        def _():
            project(block4, part)

        @pl.when((at >= late_start) & (lax.rem(k4, 2) == 1))
        def _():
            convolve(block4, part)

        @pl.when(at >= late_start)
        def _():
            @pl.loop(0, side)
            def _(pu):
                @pl.loop(0, side)
                def _(pv):
                    routes(block4, k4, pu, pv, lambda copy: copy.wait_send())

        return carry

    lax.fori_loop(0, blocks * tall + late_start, tick, 0)

    @pl.when(sp + 1 < sp_size)
    def _():
        tail.wait_send()
        docs_tail.wait_send()


def mixed_product(rows, docs, value_weight, gate_weight, conv_weight):
    side = lax.axis_size("dp") // 2
    tall = lax.axis_size("sp") // side
    count, width = rows.shape
    channels = value_weight.shape[1]
    blocks = channels // (LANES * (tall // 2))
    pieces = tall * side * side
    return pl.pallas_call(
        functools.partial(fused_kernel, side, tall, blocks),
        out_shape=jax.ShapeDtypeStruct((count, channels), jnp.bfloat16),
        in_specs=[pl.BlockSpec(memory_space=pl.ANY)] * 4
        + [pl.BlockSpec(memory_space=pltpu.VMEM)],
        out_specs=pl.BlockSpec(memory_space=pltpu.VMEM),
        scratch_shapes=[
            pltpu.VMEM((blocks, width, LANES * tall), jnp.bfloat16),
            pltpu.VMEM((HALO + count, width), jnp.bfloat16),
            pltpu.VMEM((1, LANES + count), jnp.int32),
            pltpu.VMEM((HALO, channels), jnp.float32),
            pltpu.VMEM((HALO // 8, HALO + count, LANES), jnp.float32),
            pltpu.VMEM((HALO // 8 - 1, HALO + count, LANES), jnp.float32),
            pltpu.VMEM((7, count, LANES), jnp.float32),
            pltpu.SemaphoreType.DMA((7, KEPT, pieces)),
            pltpu.SemaphoreType.DMA((blocks, pieces)),
            pltpu.SemaphoreType.DMA((blocks, pieces)),
            pltpu.SemaphoreType.DMA((blocks, tall)),
            pltpu.SemaphoreType.DMA((2,)),
            pltpu.SemaphoreType.DMA((4,)),
        ],
        compiler_params=pltpu.CompilerParams(
            collective_id=0, has_side_effects=True, vmem_limit_bytes=56 * 1024 * 1024
        ),
    )(rows, docs, value_weight, gate_weight, conv_weight)


def norm_kernel(mixed_ref, gain_ref, bias_ref, out_ref):
    wide = mixed_ref[...].astype(jnp.float32)
    center = wide - jnp.mean(wide, axis=-1, keepdims=True)
    spread = jnp.mean(center * center, axis=-1, keepdims=True)
    normed = center * lax.rsqrt(spread + 1e-06) * gain_ref[...] + bias_ref[...]
    out_ref[...] = (normed * jax.nn.sigmoid(normed)).astype(jnp.bfloat16)


def finish(mixed, norm_gain, norm_bias):
    count, channels = mixed.shape
    rows = 64
    return pl.pallas_call(
        norm_kernel,
        grid=(count // rows,),
        out_shape=jax.ShapeDtypeStruct((count, channels), jnp.bfloat16),
        in_specs=[
            pl.BlockSpec((rows, channels), lambda i: (i, 0)),
            pl.BlockSpec((1, channels), lambda i: (0, 0)),
            pl.BlockSpec((1, channels), lambda i: (0, 0)),
        ],
        out_specs=pl.BlockSpec((rows, channels), lambda i: (i, 0)),
    )(mixed, norm_gain[None], norm_bias[None])


def per_device(tokens, documents, value_weight, gate_weight, conv_weight, norm_gain, norm_bias):
    batch, count, width = tokens.shape
    channels = value_weight.shape[1]
    rows = tokens.reshape(batch * count, width)
    mixed = mixed_product(rows, documents, value_weight, gate_weight, conv_weight)
    out = finish(mixed, norm_gain, norm_bias)
    return out.reshape(batch, count, channels)


def solution(mesh):
    return jax.shard_map(
        per_device,
        mesh=mesh,
        in_specs=(
            P("dp", "sp", None),
            P("dp", "sp"),
            P(("sp", "dp"), None),
            P(("sp", "dp"), None),
            P(),
            P(),
            P(),
        ),
        out_specs=P("dp", "sp", None),
        check_vma=False,
    )
```

```python
import functools

import jax
import jax.numpy as jnp
from jax import lax
from jax.experimental import pallas as pl
from jax.experimental.pallas import tpu as pltpu
from jax.sharding import PartitionSpec as P

KERNEL = 31
HALO = 32
LANES = 128
TILE = 64
MESH = pl.DeviceIdType.MESH


def plan(side, tall, channels):
    order = dict(blocks=channels // LANES, tall_first=(0, 2, 6, 7, 11, 12), own=52)
    if side == 2 and tall == 4:
        order.update(along_z=(2, 4, 6), along_u=(0, 6, 9, 9), near_v=(17, 15, 12, 16), far_v=(12, 16, 17, 18), late=20)
    else:
        order.update(
            own=tall,
            along_z=tuple(range(1, tall)),
            along_u=tuple(range(2, tall + 2)),
            near_v=tuple(range(6, tall + 6)),
            far_v=tuple(range(6, tall + 6)),
            late=6 + tall,
        )
    return order


def fused_kernel(
    side, tall, order, tok_hbm, docs_hbm, value_hbm, gate_hbm, conv_ref, mixed_ref,
    weights, tok, docs, taps, shifted, far, near_by, send, recv, cross, own, begin, halo
):
    sp, dp = lax.axis_index("sp"), lax.axis_index("dp")
    sp_size = lax.axis_size("sp")
    core, y = lax.rem(dp, 2), lax.div(dp, 2)
    z, x = lax.div(sp, side), lax.rem(sp, side)
    flip = core == 1
    u, v = jnp.where(flip, y, x), jnp.where(flip, x, y)
    depth = value_hbm.shape[0]
    count = tok_hbm.shape[0]
    blocks = order["blocks"]
    parts = mixed_ref.shape[1] // (blocks * LANES)
    other = {"sp": sp, "dp": y * 2 + (1 - core)}
    here = (z * side + x) * side + y

    pieces = tall * side * side

    def device(dz, du, dv):
        dx, dy = jnp.where(flip, dv, du), jnp.where(flip, du, dv)
        return {"sp": dz * side + dx, "dp": dy * 2 + core}

    def number(pz, pu, pv):
        px, py = jnp.where(flip, pv, pu), jnp.where(flip, pu, pv)
        return (pz * side + px) * side + py

    def piece(which, block, q):
        return weights.at[
            block, pl.ds(pl.multiple_of((q * 2 + which) * depth, depth), depth), :
        ]

    def link(kind, block, q, target):
        return pltpu.make_async_remote_copy(
            src_ref=piece(core, block, q),
            dst_ref=piece(core, block, q),
            send_sem=send.at[kind, block],
            recv_sem=recv.at[block, q],
            device_id=target,
            device_id_type=MESH,
        )

    def hand_over(rows, block):
        return pltpu.make_async_remote_copy(
            src_ref=rows,
            dst_ref=rows,
            send_sem=send.at[6, block],
            recv_sem=cross.at[block],
            device_id=other,
            device_id_type=MESH,
        )

    def many(block, amount):
        return weights.at[block, pl.ds(0, amount * depth), :]

    def tall_first(block):
        return functools.reduce(
            jnp.logical_or, [block == chosen for chosen in order["tall_first"]]
        )

    def spread(kind, block, q, at, source, extent, target, allowed):
        if source is at:
            if extent == 2:
                ways = (((None), 1 - at, kind),)
            else:
                ways = ((at + 1 < extent, at + 1, kind), (at > 0, at - 1, kind + 1))
        elif extent == 2:
            return
        else:
            rising = at > source
            onward = jnp.where(rising, at + 1, at - 1)
            inside = (onward >= 0) & (onward < extent)
            ways = ((inside, onward, jnp.where(rising, kind, kind + 1)),)
        for taken, onward, which in ways:
            conditions = [c for c in (taken, allowed) if c is not None]
            copy = link(which, block, q, target(onward))
            if conditions:
                pl.when(functools.reduce(jnp.logical_and, conditions))(copy.start)
            else:
                copy.start()

    def pass_on(block, pz, pu, pv):
        q = number(pz, pu, pv)
        first = tall_first(block)
        if pv is v:
            along_z = None if pu is u else jnp.logical_not(first)
            spread(0, block, q, z, pz, tall, lambda to: device(to, u, v), along_z)
            along_u = None if pz is z else first
            spread(2, block, q, u, pu, side, lambda to: device(z, to, v), along_u)
        spread(4, block, q, v, pv, side, lambda to: device(z, u, to), None)
        hand_over(piece(core, block, q), block).start()

    def sent(kind, block, amount, choices):
        for chosen in choices:
            copy = pltpu.make_async_remote_copy(
                src_ref=many(block, chosen),
                dst_ref=many(block, chosen),
                send_sem=send.at[kind, block],
                recv_sem=cross.at[block],
                device_id=other,
                device_id_type=MESH,
            )
            pl.when(amount == chosen)(copy.wait_send)

    def all_sent(block):
        first = tall_first(block)
        across = jnp.where(first, 1, side)
        up = jnp.where(z + 1 < tall, (z + 1) * across, 0)
        down = jnp.where(z > 0, (tall - z) * across, 0)
        choices = sorted({n * m for n in range(1, tall + 1) for m in (1, side)})
        sent(0, block, up, choices)
        sent(1, block, down, choices)
        height = jnp.where(first, tall, 1)
        if side == 2:
            sent(2, block, height, (1, tall))
        else:
            choices = sorted({n * m for n in range(1, side + 1) for m in (1, tall)})
            sent(2, block, jnp.where(u + 1 < side, (u + 1) * height, 0), choices)
            sent(3, block, jnp.where(u > 0, (side - u) * height, 0), choices)
        plane = tall * side
        if side == 2:
            sent(4, block, jnp.int32(plane), (plane,))
        else:
            choices = [n * plane for n in range(1, side + 1)]
            sent(4, block, jnp.where(v + 1 < side, (v + 1) * plane, 0), choices)
            sent(5, block, jnp.where(v > 0, (side - v) * plane, 0), choices)
        hand_over(many(block, pieces), block).wait_send()

    def arrived(block, pz, pu, pv):
        link(0, block, number(pz, pu, pv), other).wait_recv()
        pass_on(block, pz, pu, pv)

    low = jnp.minimum(z, tall - 1 - z)

    def near(k):
        step = jnp.where(lax.rem(k, 2) == 1, low - lax.div(k + 1, 2), low + lax.div(k, 2))
        at = jnp.where(k <= 2 * low, step, k)
        return jnp.where(z == low, at, tall - 1 - at)

    def own_copies(block):
        rows = pl.ds(pl.multiple_of((here * 2 + core) * depth, depth), depth)
        for part in range(parts):
            first = pl.multiple_of((block * parts + part) * LANES, LANES)
            for half, source in enumerate((value_hbm, gate_hbm)):
                yield pltpu.make_async_copy(
                    source.at[:, pl.ds(first, LANES)],
                    weights.at[block, rows, pl.ds((2 * part + half) * LANES, LANES)],
                    own.at[block, 2 * part + half],
                )

    def send_own(block):
        for copy in own_copies(block):
            copy.wait()
        pass_on(block, z, u, v)

    @pl.loop(0, blocks)
    def _(block):
        for copy in own_copies(block):
            copy.start()

    load = pltpu.make_async_copy(tok_hbm, tok.at[pl.ds(HALO, count), :], begin.at[0])
    load.start()
    read = pltpu.make_async_copy(docs_hbm, docs.at[:, pl.ds(LANES, count)], begin.at[1])
    read.start()

    barrier = pltpu.get_barrier_semaphore()
    greeted = jnp.int32(1)
    pl.semaphore_signal(barrier, inc=1, device_id=other, device_id_type=MESH)
    for there, target in (
        (z + 1 < tall, device(z + 1, u, v)),
        (z > 0, device(z - 1, u, v)),
        (u + 1 < side, device(z, u + 1, v)),
        (u > 0, device(z, u - 1, v)),
        (v + 1 < side, device(z, u, v + 1)),
        (v > 0, device(z, u, v - 1)),
        (sp + 1 < sp_size, {"sp": sp + 1, "dp": dp}),
        (sp > 0, {"sp": sp - 1, "dp": dp}),
    ):
        greeted = greeted + there.astype(jnp.int32)

        @pl.when(there)
        def _(target=target):
            pl.semaphore_signal(barrier, inc=1, device_id=target, device_id_type=MESH)

    pl.semaphore_wait(barrier, greeted)

    following = {"sp": lax.rem(sp + 1, sp_size), "dp": dp}
    tail = pltpu.make_async_remote_copy(
        src_ref=tok_hbm.at[pl.ds(count - HALO, HALO), :],
        dst_ref=tok.at[pl.ds(0, HALO), :],
        send_sem=halo.at[0],
        recv_sem=halo.at[1],
        device_id=following,
        device_id_type=MESH,
    )
    docs_tail = pltpu.make_async_remote_copy(
        src_ref=docs_hbm.at[:, pl.ds(count - LANES, LANES)],
        dst_ref=docs.at[:, pl.ds(0, LANES)],
        send_sem=halo.at[2],
        recv_sem=halo.at[3],
        device_id=following,
        device_id_type=MESH,
    )

    ahead = min(blocks, -(-order["own"] // tall))

    @pl.loop(0, ahead)
    def _(block):
        send_own(block)

    @pl.when(sp + 1 < sp_size)
    def _():
        tail.start()
        docs_tail.start()

    @pl.when(sp == 0)
    def _():
        tok[pl.ds(0, HALO), :] = jnp.zeros((HALO, tok.shape[1]), tok.dtype)
        docs[:, pl.ds(0, LANES)] = jnp.full((1, LANES), -1, jnp.int32)

    taps[pl.ds(0, KERNEL), :] = conv_ref[...].astype(jnp.float32)

    def prepare():
        load.wait()
        read.wait()

        @pl.when(sp > 0)
        def _():
            tail.wait_recv()
            docs_tail.wait_recv()

        column = jnp.broadcast_to(docs[...], (LANES, LANES + count)).T
        wide = column[LANES - HALO :]
        for lag in range(8, HALO, 8):
            same = wide[HALO - 8 :] == wide[HALO - 8 - lag : HALO + count - lag]
            far[lag // 8 - 1, pl.ds(HALO - 8, count + 8), :] = same.astype(jnp.float32)
        for lag in range(1, 8):
            same = wide[HALO:] == wide[HALO - lag : HALO + count - lag]
            near_by[lag - 1] = same.astype(jnp.float32)

    def project(block, part):
        held = weights[
            block, :, pl.ds(pl.multiple_of(part * 2 * LANES, 2 * LANES), 2 * LANES)
        ]
        both = jnp.dot(tok[...], held, preferred_element_type=jnp.float32)
        value = both[:, :LANES].astype(jnp.bfloat16).astype(jnp.float32)
        gate = both[:, LANES:].astype(jnp.bfloat16).astype(jnp.float32)
        glu = (value * jax.nn.sigmoid(gate)).astype(jnp.bfloat16).astype(jnp.float32)
        shifted[0] = glu

    def convolve(block, part):
        first = pl.multiple_of((block * parts + part) * LANES, LANES)
        lanes = pl.ds(first, LANES)
        kept = pl.ds(HALO - 8, count + 8)
        for a in range(1, HALO // 8):
            shifted[a, kept, :] = (
                shifted[0, pl.ds(HALO - 8 - 8 * a, count + 8), :] * far[a - 1, kept, :]
            )

        @pl.loop(0, count // TILE)
        def _(tile):
            top = pl.multiple_of(tile * TILE, TILE)
            total = None
            for r in range(8):
                run = None
                for a in range(HALO // 8):
                    lag = 8 * a + r
                    if lag < KERNEL:
                        moved = shifted[a, pl.ds(top + HALO - r, TILE), :]
                        term = moved * taps[lag : lag + 1, lanes]
                        run = term if run is None else run + term
                if r:
                    run = run * near_by[r - 1, pl.ds(top, TILE), :]
                total = run if total is None else total + run
            mixed_ref[pl.ds(top, TILE), lanes] = total.astype(jnp.bfloat16)

    def level(k):
        return z if k == 0 else near(k)

    def near_u(block, k):
        @pl.loop(1, side)
        def _(du):
            arrived(block, level(k), lax.rem(u + du, side), v)

    def near_v(block, k):
        @pl.loop(1, side)
        def _(dv):
            arrived(block, level(k), u, lax.rem(v + dv, side))

    def far_v(block, k):
        @pl.loop(1, side)
        def _(du):
            @pl.loop(1, side)
            def _(dv):
                arrived(block, level(k), lax.rem(u + du, side), lax.rem(v + dv, side))

    def compute(block, k):
        if k == 0:
            hand_over(many(block, pieces), block).wait_recv()

        for step in range(k * 2 * parts // tall, (k + 1) * 2 * parts // tall):
            if step % 2 == 0:
                project(block, step // 2)
            else:
                convolve(block, step // 2)

        if k == tall - 1:
            all_sent(block)

    sites = [(-order["own"], lambda block: send_own(block))]
    for k in range(1, tall):
        sites.append((order["along_z"][k - 1], lambda block, k=k: arrived(block, near(k), u, v)))
    for name, act in (("along_u", near_u), ("near_v", near_v), ("far_v", far_v)):
        for k in range(tall):
            sites.append((order[name][k], lambda block, k=k, act=act: act(block, k)))
    for k in range(tall):
        sites.append((order["late"] + k, lambda block, k=k: compute(block, k)))
    assert all(offset <= order["late"] for offset, _ in sites[:-tall])

    def round_of(number, carry):
        for j in range(tall):
            for offset, act in sites:
                if offset % tall != j:
                    continue
                block = number - offset // tall
                first = ahead if offset < 0 else 0

                @pl.when((block >= first) & (block < blocks))
                def _(block=block, act=act):
                    act(block)

        return carry

    prepare()
    rounds = blocks + (order["late"] + tall - 1) // tall
    lax.fori_loop(0, rounds, round_of, 0)

    @pl.when(sp + 1 < sp_size)
    def _():
        tail.wait_send()
        docs_tail.wait_send()


def mixed_product(rows, docs, value_weight, gate_weight, conv_weight):
    side = lax.axis_size("dp") // 2
    tall = lax.axis_size("sp") // side
    count, width = rows.shape
    channels = value_weight.shape[1]
    order = plan(side, tall, channels)
    blocks = order["blocks"]
    pieces = tall * side * side
    return pl.pallas_call(
        functools.partial(fused_kernel, side, tall, order),
        out_shape=jax.ShapeDtypeStruct((count, channels), jnp.bfloat16),
        in_specs=[pl.BlockSpec(memory_space=pl.ANY)] * 4
        + [pl.BlockSpec(memory_space=pltpu.VMEM)],
        out_specs=pl.BlockSpec(memory_space=pltpu.VMEM),
        scratch_shapes=[
            pltpu.VMEM((blocks, width, 2 * channels // blocks), jnp.bfloat16),
            pltpu.VMEM((HALO + count, width), jnp.bfloat16),
            pltpu.VMEM((1, LANES + count), jnp.int32),
            pltpu.VMEM((HALO, channels), jnp.float32),
            pltpu.VMEM((HALO // 8, HALO + count, LANES), jnp.float32),
            pltpu.VMEM((HALO // 8 - 1, HALO + count, LANES), jnp.float32),
            pltpu.VMEM((7, count, LANES), jnp.float32),
            pltpu.SemaphoreType.DMA((7, blocks)),
            pltpu.SemaphoreType.DMA((blocks, pieces)),
            pltpu.SemaphoreType.DMA((blocks,)),
            pltpu.SemaphoreType.DMA((blocks, 2 * channels // (blocks * LANES))),
            pltpu.SemaphoreType.DMA((2,)),
            pltpu.SemaphoreType.DMA((4,)),
        ],
        compiler_params=pltpu.CompilerParams(
            collective_id=0, has_side_effects=True, vmem_limit_bytes=56 * 1024 * 1024
        ),
    )(rows, docs, value_weight, gate_weight, conv_weight)


def norm_kernel(mixed_ref, gain_ref, bias_ref, out_ref):
    wide = mixed_ref[...].astype(jnp.float32)
    center = wide - jnp.mean(wide, axis=-1, keepdims=True)
    spread = jnp.mean(center * center, axis=-1, keepdims=True)
    normed = center * lax.rsqrt(spread + 1e-06) * gain_ref[...] + bias_ref[...]
    out_ref[...] = (normed * jax.nn.sigmoid(normed)).astype(jnp.bfloat16)


def finish(mixed, norm_gain, norm_bias):
    count, channels = mixed.shape
    rows = 64
    return pl.pallas_call(
        norm_kernel,
        grid=(count // rows,),
        out_shape=jax.ShapeDtypeStruct((count, channels), jnp.bfloat16),
        in_specs=[
            pl.BlockSpec((rows, channels), lambda i: (i, 0)),
            pl.BlockSpec((1, channels), lambda i: (0, 0)),
            pl.BlockSpec((1, channels), lambda i: (0, 0)),
        ],
        out_specs=pl.BlockSpec((rows, channels), lambda i: (i, 0)),
    )(mixed, norm_gain[None], norm_bias[None])


def per_device(tokens, documents, value_weight, gate_weight, conv_weight, norm_gain, norm_bias):
    batch, count, width = tokens.shape
    channels = value_weight.shape[1]
    rows = tokens.reshape(batch * count, width)
    mixed = mixed_product(rows, documents, value_weight, gate_weight, conv_weight)
    out = finish(mixed, norm_gain, norm_bias)
    return out.reshape(batch, count, channels)


def solution(mesh):
    return jax.shard_map(
        per_device,
        mesh=mesh,
        in_specs=(
            P("dp", "sp", None),
            P("dp", "sp"),
            P(("sp", "dp"), None),
            P(("sp", "dp"), None),
            P(),
            P(),
            P(),
        ),
        out_specs=P("dp", "sp", None),
        check_vma=False,
    )
```

```python
import functools

import jax
import jax.numpy as jnp
from jax import lax
from jax.experimental import pallas as pl
from jax.experimental.pallas import tpu as pltpu
from jax.sharding import PartitionSpec as P

KERNEL = 31
HALO = 32
LANES = 128
TILE = 128
SPARE = 8
LEAVE = 32
MESH = pl.DeviceIdType.MESH


def plan(side, tall, channels):
    order = dict(blocks=channels // LANES, tall_first=(1, 4, 7, 10, 13), own=20)
    if side == 2 and tall == 4:
        order.update(along_z=(0, 4, 7), along_u=(0, 7, 8, 10), near_v=(3, 9, 11, 11), far_v=(9, 13, 13, 13), late=15)
    else:
        order.update(
            own=tall,
            along_z=tuple(range(1, tall)),
            along_u=tuple(range(2, tall + 2)),
            near_v=tuple(range(6, tall + 6)),
            far_v=tuple(range(6, tall + 6)),
            late=6 + tall,
        )
    return order


def fused_kernel(
    side, tall, order, tok_hbm, docs_hbm, value_hbm, gate_hbm, conv_ref, gain_ref,
    bias_ref, out_hbm, weights, tok, docs, taps, shifted, far, near_by, mixed, center,
    total, square, send, recv, cross, own, begin, halo, leave
):
    sp, dp = lax.axis_index("sp"), lax.axis_index("dp")
    sp_size = lax.axis_size("sp")
    core, y = lax.rem(dp, 2), lax.div(dp, 2)
    z, x = lax.div(sp, side), lax.rem(sp, side)
    flip = core == 1
    u, v = jnp.where(flip, y, x), jnp.where(flip, x, y)
    depth = value_hbm.shape[0]
    count = tok_hbm.shape[0]
    blocks = order["blocks"]
    channels = value_hbm.shape[1]
    parts = channels // (blocks * LANES)
    lines = (HALO + count) // 2
    other = {"sp": sp, "dp": y * 2 + (1 - core)}
    here = (z * side + x) * side + y

    pieces = tall * side * side

    def device(dz, du, dv):
        dx, dy = jnp.where(flip, dv, du), jnp.where(flip, du, dv)
        return {"sp": dz * side + dx, "dp": dy * 2 + core}

    def number(pz, pu, pv):
        px, py = jnp.where(flip, pv, pu), jnp.where(flip, pu, pv)
        return (pz * side + px) * side + py

    def piece(which, block, q):
        return weights.at[
            block, pl.ds(pl.multiple_of((q * 2 + which) * depth, depth), depth), :
        ]

    def link(kind, block, q, target):
        return pltpu.make_async_remote_copy(
            src_ref=piece(core, block, q),
            dst_ref=piece(core, block, q),
            send_sem=send.at[kind, block],
            recv_sem=recv.at[block, q],
            device_id=target,
            device_id_type=MESH,
        )

    def hand_over(rows, block):
        return pltpu.make_async_remote_copy(
            src_ref=rows,
            dst_ref=rows,
            send_sem=send.at[6, block],
            recv_sem=cross.at[block],
            device_id=other,
            device_id_type=MESH,
        )

    def many(block, amount):
        return weights.at[block, pl.ds(0, amount * depth), :]

    def tall_first(block):
        return functools.reduce(
            jnp.logical_or, [block == chosen for chosen in order["tall_first"]]
        )

    def spread(kind, block, q, at, source, extent, target, allowed):
        if source is at:
            if extent == 2:
                ways = (((None), 1 - at, kind),)
            else:
                ways = ((at + 1 < extent, at + 1, kind), (at > 0, at - 1, kind + 1))
        elif extent == 2:
            return
        else:
            rising = at > source
            onward = jnp.where(rising, at + 1, at - 1)
            inside = (onward >= 0) & (onward < extent)
            ways = ((inside, onward, jnp.where(rising, kind, kind + 1)),)
        for taken, onward, which in ways:
            conditions = [c for c in (taken, allowed) if c is not None]
            copy = link(which, block, q, target(onward))
            if conditions:
                pl.when(functools.reduce(jnp.logical_and, conditions))(copy.start)
            else:
                copy.start()

    def pass_on(block, pz, pu, pv):
        q = number(pz, pu, pv)
        first = tall_first(block)
        if pv is v:
            along_z = None if pu is u else jnp.logical_not(first)
            spread(0, block, q, z, pz, tall, lambda to: device(to, u, v), along_z)
            along_u = None if pz is z else first
            spread(2, block, q, u, pu, side, lambda to: device(z, to, v), along_u)
        spread(4, block, q, v, pv, side, lambda to: device(z, u, to), None)
        hand_over(piece(core, block, q), block).start()

    def sent(kind, block, amount, choices):
        for chosen in choices:
            copy = pltpu.make_async_remote_copy(
                src_ref=many(block, chosen),
                dst_ref=many(block, chosen),
                send_sem=send.at[kind, block],
                recv_sem=cross.at[block],
                device_id=other,
                device_id_type=MESH,
            )
            pl.when(amount == chosen)(copy.wait_send)

    def all_sent(block):
        first = tall_first(block)
        across = jnp.where(first, 1, side)
        up = jnp.where(z + 1 < tall, (z + 1) * across, 0)
        down = jnp.where(z > 0, (tall - z) * across, 0)
        choices = sorted({n * m for n in range(1, tall + 1) for m in (1, side)})
        sent(0, block, up, choices)
        sent(1, block, down, choices)
        height = jnp.where(first, tall, 1)
        if side == 2:
            sent(2, block, height, (1, tall))
        else:
            choices = sorted({n * m for n in range(1, side + 1) for m in (1, tall)})
            sent(2, block, jnp.where(u + 1 < side, (u + 1) * height, 0), choices)
            sent(3, block, jnp.where(u > 0, (side - u) * height, 0), choices)
        plane = tall * side
        if side == 2:
            sent(4, block, jnp.int32(plane), (plane,))
        else:
            choices = [n * plane for n in range(1, side + 1)]
            sent(4, block, jnp.where(v + 1 < side, (v + 1) * plane, 0), choices)
            sent(5, block, jnp.where(v > 0, (side - v) * plane, 0), choices)
        hand_over(many(block, pieces), block).wait_send()

    def arrived(block, pz, pu, pv):
        link(0, block, number(pz, pu, pv), other).wait_recv()
        pass_on(block, pz, pu, pv)

    low = jnp.minimum(z, tall - 1 - z)

    def near(k):
        step = jnp.where(lax.rem(k, 2) == 1, low - lax.div(k + 1, 2), low + lax.div(k, 2))
        at = jnp.where(k <= 2 * low, step, k)
        return jnp.where(z == low, at, tall - 1 - at)

    def own_copies(block):
        rows = pl.ds(pl.multiple_of((here * 2 + core) * depth, depth), depth)
        for part in range(parts):
            first = pl.multiple_of((block * parts + part) * LANES, LANES)
            for half, source in enumerate((value_hbm, gate_hbm)):
                yield pltpu.make_async_copy(
                    source.at[:, pl.ds(first, LANES)],
                    weights.at[block, rows, pl.ds((2 * part + half) * LANES, LANES)],
                    own.at[block, 2 * part + half],
                )

    def send_own(block):
        for copy in own_copies(block):
            copy.wait()
        pass_on(block, z, u, v)

    barrier = pltpu.get_barrier_semaphore()
    greeted = jnp.int32(1)
    pl.semaphore_signal(barrier, inc=1, device_id=other, device_id_type=MESH)
    for there, target in (
        (z + 1 < tall, device(z + 1, u, v)),
        (z > 0, device(z - 1, u, v)),
        (u + 1 < side, device(z, u + 1, v)),
        (u > 0, device(z, u - 1, v)),
        (v + 1 < side, device(z, u, v + 1)),
        (v > 0, device(z, u, v - 1)),
        (sp + 1 < sp_size, {"sp": sp + 1, "dp": dp}),
        (sp > 0, {"sp": sp - 1, "dp": dp}),
    ):
        greeted = greeted + there.astype(jnp.int32)

        @pl.when(there)
        def _(target=target):
            pl.semaphore_signal(barrier, inc=1, device_id=target, device_id_type=MESH)

    @pl.loop(0, blocks)
    def _(block):
        for copy in own_copies(block):
            copy.start()

    load = pltpu.make_async_copy(tok_hbm, tok.at[pl.ds(HALO, count), :], begin.at[0])
    load.start()
    read = pltpu.make_async_copy(docs_hbm, docs.at[:, pl.ds(LANES, count)], begin.at[1])
    read.start()

    pl.semaphore_wait(barrier, greeted)

    following = {"sp": lax.rem(sp + 1, sp_size), "dp": dp}
    tail = pltpu.make_async_remote_copy(
        src_ref=tok_hbm.at[pl.ds(count - HALO, HALO), :],
        dst_ref=tok.at[pl.ds(0, HALO), :],
        send_sem=halo.at[0],
        recv_sem=halo.at[1],
        device_id=following,
        device_id_type=MESH,
    )
    docs_tail = pltpu.make_async_remote_copy(
        src_ref=docs_hbm.at[:, pl.ds(count - LANES, LANES)],
        dst_ref=docs.at[:, pl.ds(0, LANES)],
        send_sem=halo.at[2],
        recv_sem=halo.at[3],
        device_id=following,
        device_id_type=MESH,
    )

    @pl.when(sp + 1 < sp_size)
    def _():
        tail.start()
        docs_tail.start()

    ahead = min(blocks, -(-order["own"] // tall))

    @pl.loop(0, ahead)
    def _(block):
        send_own(block)

    @pl.when(sp == 0)
    def _():
        tok[pl.ds(0, HALO), :] = jnp.zeros((HALO, tok.shape[1]), tok.dtype)
        docs[:, pl.ds(0, LANES)] = jnp.full((1, LANES), -1, jnp.int32)

    taps[pl.ds(0, KERNEL), :] = conv_ref[...].astype(jnp.float32)

    def prepare():
        load.wait()
        read.wait()

        @pl.when(sp > 0)
        def _():
            tail.wait_recv()
            docs_tail.wait_recv()

        column = jnp.broadcast_to(docs[...], (LANES, LANES + count)).T
        wide = column[LANES - HALO :]
        for lag in range(8, HALO, 8):
            same = wide[HALO - 8 :] == wide[HALO - 8 - lag : HALO + count - lag]
            far[lag // 8 - 1, pl.ds(HALO - 8, count + 8), :] = same.astype(jnp.float32)
        for lag in range(1, 8):
            same = wide[HALO:] == wide[HALO - lag : HALO + count - lag]
            near_by[lag - 1, pl.ds(0, count), :] = same.astype(jnp.float32)

        total[...] = jnp.zeros_like(total)
        square[...] = jnp.zeros_like(square)

    def project(block, part, half):
        rows = pl.ds(half * lines, lines)
        held = weights[
            block, :, pl.ds(pl.multiple_of(part * 2 * LANES, 2 * LANES), 2 * LANES)
        ]
        both = jnp.dot(tok[rows, :], held, preferred_element_type=jnp.float32)
        value = both[:, :LANES].astype(jnp.bfloat16).astype(jnp.float32)
        gate = both[:, LANES:].astype(jnp.bfloat16).astype(jnp.float32)
        glu = (value * jax.nn.sigmoid(gate)).astype(jnp.bfloat16).astype(jnp.float32)
        shifted[0, rows, :] = glu

    def convolve(block, part, half):
        first = pl.multiple_of((block * parts + part) * LANES, LANES)
        lanes = pl.ds(first, LANES)
        span = count // 2
        start = half * span + HALO - 8
        kept = pl.ds(start, span + 8)
        for a in range(1, HALO // 8):
            moved = shifted[0, pl.ds(start - 8 * a, span + 8), :]
            shifted[a, kept, :] = moved * far[a - 1, kept, :]

        @pl.loop(0, span // TILE)
        def _(tile):
            top = pl.multiple_of(half * span + tile * TILE, TILE)
            held = None
            for r in range(8):
                run = None
                for a in range(HALO // 8):
                    lag = 8 * a + r
                    if lag < KERNEL:
                        moved = shifted[a, pl.ds(top + HALO - r, TILE), :]
                        term = moved * taps[lag : lag + 1, lanes]
                        run = term if run is None else run + term
                if r:
                    run = run * near_by[r - 1, pl.ds(top, TILE), :]
                held = run if held is None else held + run
            rows = pl.ds(top, TILE)
            rounded = held.astype(jnp.bfloat16)
            mixed[rows, lanes] = rounded
            held = rounded.astype(jnp.float32)

            @pl.when(first == 0)
            def _():
                middle = jnp.mean(held, axis=-1, keepdims=True)
                center[rows, :] = jnp.broadcast_to(middle, (TILE, LANES))

            off = held - center[rows, :]
            total[rows, :] += off
            square[rows, :] += off * off

    def leaving(step):
        rows = pl.ds(pl.multiple_of(step * LEAVE, LEAVE), LEAVE)
        return pltpu.make_async_copy(mixed.at[rows, :], out_hbm.at[rows, :], leave.at[step])

    def finish():
        moved = jnp.sum(total[...], axis=-1, keepdims=True) / channels
        spread = jnp.sum(square[...], axis=-1, keepdims=True) / channels - moved * moved
        scale = lax.rsqrt(jnp.maximum(spread, 0.0) + 1e-06)
        center[...] = center[...] + moved
        total[...] = jnp.broadcast_to(scale, total.shape)

        @pl.loop(0, count // LEAVE)
        def _(step):
            rows = pl.ds(pl.multiple_of(step * LEAVE, LEAVE), LEAVE)
            middle, scale = center[rows, :], total[rows, :]
            for lane in range(0, channels, LANES):
                lanes = pl.ds(lane, LANES)
                wide = mixed[rows, lanes].astype(jnp.float32)
                normed = (wide - middle) * scale * gain_ref[:, lanes] + bias_ref[:, lanes]
                mixed[rows, lanes] = (normed * jax.nn.sigmoid(normed)).astype(jnp.bfloat16)
            leaving(step).start()

        @pl.loop(0, count // LEAVE)
        def _(step):
            leaving(step).wait()

    def level(k):
        return z if k == 0 else near(k)

    def near_u(block, k):
        @pl.loop(1, side)
        def _(du):
            arrived(block, level(k), lax.rem(u + du, side), v)

    def near_v(block, k):
        @pl.loop(1, side)
        def _(dv):
            arrived(block, level(k), u, lax.rem(v + dv, side))

    def far_v(block, k):
        @pl.loop(1, side)
        def _(du):
            @pl.loop(1, side)
            def _(dv):
                arrived(block, level(k), lax.rem(u + du, side), lax.rem(v + dv, side))

    def compute(block, k):
        if k == 0:
            pl.when(block == 0)(prepare)
            hand_over(many(block, pieces), block).wait_recv()

        steps = [
            (act, part, half)
            for part in range(parts)
            for act in (project, convolve)
            for half in range(2)
        ]
        for act, part, half in steps[k * len(steps) // tall : (k + 1) * len(steps) // tall]:
            act(block, part, half)

        if k == tall - 1:
            all_sent(block)

    sites = [(-order["own"], lambda block: send_own(block))]
    for k in range(1, tall):
        sites.append((order["along_z"][k - 1], lambda block, k=k: arrived(block, near(k), u, v)))
    for name, act in (("along_u", near_u), ("near_v", near_v), ("far_v", far_v)):
        for k in range(tall):
            sites.append((order[name][k], lambda block, k=k, act=act: act(block, k)))
    for k in range(tall):
        sites.append((order["late"] + k, lambda block, k=k: compute(block, k)))
    assert all(offset <= order["late"] for offset, _ in sites[:-tall])

    def round_of(number, carry):
        for j in range(tall):
            for offset, act in sites:
                if offset % tall != j:
                    continue
                block = number - offset // tall
                first = ahead if offset < 0 else 0

                @pl.when((block >= first) & (block < blocks))
                def _(block=block, act=act):
                    act(block)

        return carry

    rounds = blocks + (order["late"] + tall - 1) // tall
    lax.fori_loop(0, rounds, round_of, 0)
    finish()

    @pl.when(sp + 1 < sp_size)
    def _():
        tail.wait_send()
        docs_tail.wait_send()


def activated_product(
    rows, docs, value_weight, gate_weight, conv_weight, norm_gain, norm_bias
):
    side = lax.axis_size("dp") // 2
    tall = lax.axis_size("sp") // side
    count, width = rows.shape
    channels = value_weight.shape[1]
    order = plan(side, tall, channels)
    blocks = order["blocks"]
    pieces = tall * side * side
    return pl.pallas_call(
        functools.partial(fused_kernel, side, tall, order),
        out_shape=jax.ShapeDtypeStruct((count, channels), jnp.bfloat16),
        in_specs=[pl.BlockSpec(memory_space=pl.ANY)] * 4
        + [pl.BlockSpec(memory_space=pltpu.VMEM)] * 3,
        out_specs=pl.BlockSpec(memory_space=pl.ANY),
        scratch_shapes=[
            pltpu.VMEM((blocks, width, 2 * channels // blocks), jnp.bfloat16),
            pltpu.VMEM((HALO + count, width), jnp.bfloat16),
            pltpu.VMEM((1, LANES + count), jnp.int32),
            pltpu.VMEM((HALO, channels), jnp.float32),
            pltpu.VMEM((HALO // 8, HALO + count + SPARE, LANES), jnp.float32),
            pltpu.VMEM((HALO // 8 - 1, HALO + count + SPARE, LANES), jnp.float32),
            pltpu.VMEM((7, count + SPARE, LANES), jnp.float32),
            pltpu.VMEM((count, channels), jnp.bfloat16),
            pltpu.VMEM((count, LANES), jnp.float32),
            pltpu.VMEM((count, LANES), jnp.float32),
            pltpu.VMEM((count, LANES), jnp.float32),
            pltpu.SemaphoreType.DMA((7, blocks)),
            pltpu.SemaphoreType.DMA((blocks, pieces)),
            pltpu.SemaphoreType.DMA((blocks,)),
            pltpu.SemaphoreType.DMA((blocks, 2 * channels // (blocks * LANES))),
            pltpu.SemaphoreType.DMA((2,)),
            pltpu.SemaphoreType.DMA((4,)),
            pltpu.SemaphoreType.DMA((count // LEAVE,)),
        ],
        compiler_params=pltpu.CompilerParams(
            collective_id=0, has_side_effects=True, vmem_limit_bytes=56 * 1024 * 1024
        ),
    )(
        rows, docs, value_weight, gate_weight, conv_weight, norm_gain[None], norm_bias[None]
    )


def per_device(tokens, documents, value_weight, gate_weight, conv_weight, norm_gain, norm_bias):
    batch, count, width = tokens.shape
    channels = value_weight.shape[1]
    rows = tokens.reshape(batch * count, width)
    out = activated_product(
        rows, documents, value_weight, gate_weight, conv_weight, norm_gain, norm_bias
    )
    return out.reshape(batch, count, channels)


def solution(mesh):
    return jax.shard_map(
        per_device,
        mesh=mesh,
        in_specs=(
            P("dp", "sp", None),
            P("dp", "sp"),
            P(("sp", "dp"), None),
            P(("sp", "dp"), None),
            P(),
            P(),
            P(),
        ),
        out_specs=P("dp", "sp", None),
        check_vma=False,
    )
```

```python
import functools

import jax
import jax.numpy as jnp
from jax import lax
from jax.experimental import pallas as pl
from jax.experimental.pallas import tpu as pltpu
from jax.sharding import PartitionSpec as P

KERNEL = 31
HALO = 32
LANES = 128
TILE = 128
SPARE = 8
LEAVE = 32
MESH = pl.DeviceIdType.MESH


def plan(side, tall, channels):
    order = dict(blocks=channels // LANES, tall_first=((1, 4, 7, 10, 13), (0, 2, 7, 8, 11, 13)), own=47)
    if side == 2 and tall == 4:
        order.update(along_z=(0, 4, 7), along_u=(0, 7, 9, 10), near_v=(5, 11, 12, 12), far_v=(9, 13, 14, 14), late=16)
    else:
        order.update(
            own=tall,
            along_z=tuple(range(1, tall)),
            along_u=tuple(range(2, tall + 2)),
            near_v=tuple(range(6, tall + 6)),
            far_v=tuple(range(6, tall + 6)),
            late=6 + tall,
        )
    return order


def fused_kernel(
    side, tall, order, tok_hbm, docs_hbm, value_hbm, gate_hbm, conv_ref, gain_ref,
    bias_ref, mixed, weights, tok, docs, taps, shifted, far, near_by, center,
    total, square, send, recv, cross, own, begin, halo
):
    sp, dp = lax.axis_index("sp"), lax.axis_index("dp")
    sp_size = lax.axis_size("sp")
    core, y = lax.rem(dp, 2), lax.div(dp, 2)
    z, x = lax.div(sp, side), lax.rem(sp, side)
    flip = core == 1
    u, v = jnp.where(flip, y, x), jnp.where(flip, x, y)
    depth = value_hbm.shape[0]
    count = tok_hbm.shape[0]
    blocks = order["blocks"]
    channels = value_hbm.shape[1]
    parts = channels // (blocks * LANES)
    lines = (HALO + count) // 2
    other = {"sp": sp, "dp": y * 2 + (1 - core)}
    here = (z * side + x) * side + y

    pieces = tall * side * side

    def device(dz, du, dv):
        dx, dy = jnp.where(flip, dv, du), jnp.where(flip, du, dv)
        return {"sp": dz * side + dx, "dp": dy * 2 + core}

    def number(pz, pu, pv):
        px, py = jnp.where(flip, pv, pu), jnp.where(flip, pu, pv)
        return (pz * side + px) * side + py

    def piece(which, block, q):
        return weights.at[
            block, pl.ds(pl.multiple_of((q * 2 + which) * depth, depth), depth), :
        ]

    def link(kind, block, q, target):
        return pltpu.make_async_remote_copy(
            src_ref=piece(core, block, q),
            dst_ref=piece(core, block, q),
            send_sem=send.at[kind, block],
            recv_sem=recv.at[block, q],
            device_id=target,
            device_id_type=MESH,
        )

    def hand_over(rows, block):
        return pltpu.make_async_remote_copy(
            src_ref=rows,
            dst_ref=rows,
            send_sem=send.at[6, block],
            recv_sem=cross.at[block],
            device_id=other,
            device_id_type=MESH,
        )

    def many(block, amount):
        return weights.at[block, pl.ds(0, amount * depth), :]

    def tall_first(block):
        return functools.reduce(
            jnp.logical_or,
            [
                (core == which) & (block == chosen)
                for which in range(2)
                for chosen in order["tall_first"][which]
            ],
        )

    def spread(kind, block, q, at, source, extent, target, allowed):
        if source is at:
            if extent == 2:
                ways = (((None), 1 - at, kind),)
            else:
                ways = ((at + 1 < extent, at + 1, kind), (at > 0, at - 1, kind + 1))
        elif extent == 2:
            return
        else:
            rising = at > source
            onward = jnp.where(rising, at + 1, at - 1)
            inside = (onward >= 0) & (onward < extent)
            ways = ((inside, onward, jnp.where(rising, kind, kind + 1)),)
        for taken, onward, which in ways:
            conditions = [c for c in (taken, allowed) if c is not None]
            copy = link(which, block, q, target(onward))
            if conditions:
                pl.when(functools.reduce(jnp.logical_and, conditions))(copy.start)
            else:
                copy.start()

    def pass_on(block, pz, pu, pv):
        q = number(pz, pu, pv)
        first = tall_first(block)
        if pv is v:
            along_z = None if pu is u else jnp.logical_not(first)
            spread(0, block, q, z, pz, tall, lambda to: device(to, u, v), along_z)
            along_u = None if pz is z else first
            spread(2, block, q, u, pu, side, lambda to: device(z, to, v), along_u)
        spread(4, block, q, v, pv, side, lambda to: device(z, u, to), None)
        hand_over(piece(core, block, q), block).start()

    def sent(kind, block, amount, choices):
        for chosen in choices:
            copy = pltpu.make_async_remote_copy(
                src_ref=many(block, chosen),
                dst_ref=many(block, chosen),
                send_sem=send.at[kind, block],
                recv_sem=cross.at[block],
                device_id=other,
                device_id_type=MESH,
            )
            pl.when(amount == chosen)(copy.wait_send)

    def all_sent(block):
        first = tall_first(block)
        across = jnp.where(first, 1, side)
        up = jnp.where(z + 1 < tall, (z + 1) * across, 0)
        down = jnp.where(z > 0, (tall - z) * across, 0)
        choices = sorted({n * m for n in range(1, tall + 1) for m in (1, side)})
        sent(0, block, up, choices)
        sent(1, block, down, choices)
        height = jnp.where(first, tall, 1)
        if side == 2:
            sent(2, block, height, (1, tall))
        else:
            choices = sorted({n * m for n in range(1, side + 1) for m in (1, tall)})
            sent(2, block, jnp.where(u + 1 < side, (u + 1) * height, 0), choices)
            sent(3, block, jnp.where(u > 0, (side - u) * height, 0), choices)
        plane = tall * side
        if side == 2:
            sent(4, block, jnp.int32(plane), (plane,))
        else:
            choices = [n * plane for n in range(1, side + 1)]
            sent(4, block, jnp.where(v + 1 < side, (v + 1) * plane, 0), choices)
            sent(5, block, jnp.where(v > 0, (side - v) * plane, 0), choices)
        hand_over(many(block, pieces), block).wait_send()

    def arrived(block, pz, pu, pv):
        link(0, block, number(pz, pu, pv), other).wait_recv()
        pass_on(block, pz, pu, pv)

    low = jnp.minimum(z, tall - 1 - z)

    def near(k):
        step = jnp.where(lax.rem(k, 2) == 1, low - lax.div(k + 1, 2), low + lax.div(k, 2))
        at = jnp.where(k <= 2 * low, step, k)
        return jnp.where(z == low, at, tall - 1 - at)

    def own_copies(block):
        rows = pl.ds(pl.multiple_of((here * 2 + core) * depth, depth), depth)
        for part in range(parts):
            first = pl.multiple_of((block * parts + part) * LANES, LANES)
            for half, source in enumerate((value_hbm, gate_hbm)):
                yield pltpu.make_async_copy(
                    source.at[:, pl.ds(first, LANES)],
                    weights.at[block, rows, pl.ds((2 * part + half) * LANES, LANES)],
                    own.at[block, 2 * part + half],
                )

    def send_own(block):
        for copy in own_copies(block):
            copy.wait()
        pass_on(block, z, u, v)

    barrier = pltpu.get_barrier_semaphore()
    greeted = jnp.int32(1)
    pl.semaphore_signal(barrier, inc=1, device_id=other, device_id_type=MESH)
    for there, target in (
        (z + 1 < tall, device(z + 1, u, v)),
        (z > 0, device(z - 1, u, v)),
        (u + 1 < side, device(z, u + 1, v)),
        (u > 0, device(z, u - 1, v)),
        (v + 1 < side, device(z, u, v + 1)),
        (v > 0, device(z, u, v - 1)),
        (sp + 1 < sp_size, {"sp": sp + 1, "dp": dp}),
        (sp > 0, {"sp": sp - 1, "dp": dp}),
    ):
        greeted = greeted + there.astype(jnp.int32)

        @pl.when(there)
        def _(target=target):
            pl.semaphore_signal(barrier, inc=1, device_id=target, device_id_type=MESH)

    @pl.loop(0, blocks)
    def _(block):
        for copy in own_copies(block):
            copy.start()

    load = pltpu.make_async_copy(tok_hbm, tok.at[pl.ds(HALO, count), :], begin.at[0])
    load.start()
    read = pltpu.make_async_copy(docs_hbm, docs.at[:, pl.ds(LANES, count)], begin.at[1])
    read.start()

    pl.semaphore_wait(barrier, greeted)

    following = {"sp": lax.rem(sp + 1, sp_size), "dp": dp}
    tail = pltpu.make_async_remote_copy(
        src_ref=tok_hbm.at[pl.ds(count - HALO, HALO), :],
        dst_ref=tok.at[pl.ds(0, HALO), :],
        send_sem=halo.at[0],
        recv_sem=halo.at[1],
        device_id=following,
        device_id_type=MESH,
    )
    docs_tail = pltpu.make_async_remote_copy(
        src_ref=docs_hbm.at[:, pl.ds(count - LANES, LANES)],
        dst_ref=docs.at[:, pl.ds(0, LANES)],
        send_sem=halo.at[2],
        recv_sem=halo.at[3],
        device_id=following,
        device_id_type=MESH,
    )

    @pl.when(sp + 1 < sp_size)
    def _():
        tail.start()
        docs_tail.start()

    ahead = min(blocks, -(-order["own"] // tall))

    @pl.loop(0, ahead)
    def _(block):
        send_own(block)

    @pl.when(sp == 0)
    def _():
        tok[pl.ds(0, HALO), :] = jnp.zeros((HALO, tok.shape[1]), tok.dtype)
        docs[:, pl.ds(0, LANES)] = jnp.full((1, LANES), -1, jnp.int32)

    taps[pl.ds(0, KERNEL), :] = conv_ref[...].astype(jnp.float32)

    def prepare():
        load.wait()
        read.wait()

        @pl.when(sp > 0)
        def _():
            tail.wait_recv()
            docs_tail.wait_recv()

        column = jnp.broadcast_to(docs[...], (LANES, LANES + count)).T
        wide = column[LANES - HALO :]
        for lag in range(8, HALO, 8):
            same = wide[HALO - 8 :] == wide[HALO - 8 - lag : HALO + count - lag]
            far[lag // 8 - 1, pl.ds(HALO - 8, count + 8), :] = same.astype(jnp.float32)
        for lag in range(1, 8):
            same = wide[HALO:] == wide[HALO - lag : HALO + count - lag]
            near_by[lag - 1, pl.ds(0, count), :] = same.astype(jnp.float32)

        total[...] = jnp.zeros_like(total)
        square[...] = jnp.zeros_like(square)

    def project(block, part, half):
        rows = pl.ds(half * lines, lines)
        held = weights[
            block, :, pl.ds(pl.multiple_of(part * 2 * LANES, 2 * LANES), 2 * LANES)
        ]
        both = jnp.dot(tok[rows, :], held, preferred_element_type=jnp.float32)
        value = both[:, :LANES].astype(jnp.bfloat16).astype(jnp.float32)
        gate = both[:, LANES:].astype(jnp.bfloat16).astype(jnp.float32)
        glu = (value * jax.nn.sigmoid(gate)).astype(jnp.bfloat16).astype(jnp.float32)
        shifted[0, rows, :] = glu

    def convolve(block, part, half):
        first = pl.multiple_of((block * parts + part) * LANES, LANES)
        lanes = pl.ds(first, LANES)
        span = count // 2
        start = half * span + HALO - 8
        kept = pl.ds(start, span + 8)
        for a in range(1, HALO // 8):
            moved = shifted[0, pl.ds(start - 8 * a, span + 8), :]
            shifted[a, kept, :] = moved * far[a - 1, kept, :]

        @pl.loop(0, span // TILE)
        def _(tile):
            top = pl.multiple_of(half * span + tile * TILE, TILE)
            held = None
            for r in range(8):
                run = None
                for a in range(HALO // 8):
                    lag = 8 * a + r
                    if lag < KERNEL:
                        moved = shifted[a, pl.ds(top + HALO - r, TILE), :]
                        term = moved * taps[lag : lag + 1, lanes]
                        run = term if run is None else run + term
                if r:
                    run = run * near_by[r - 1, pl.ds(top, TILE), :]
                held = run if held is None else held + run
            rows = pl.ds(top, TILE)
            rounded = held.astype(jnp.bfloat16)
            mixed[rows, lanes] = rounded
            held = rounded.astype(jnp.float32)

            @pl.when(first == 0)
            def _():
                middle = jnp.mean(held, axis=-1, keepdims=True)
                center[rows, :] = jnp.broadcast_to(middle, (TILE, LANES))

            off = held - center[rows, :]
            total[rows, :] += off
            square[rows, :] += off * off

    def finish():
        moved = jnp.sum(total[...], axis=-1, keepdims=True) / channels
        spread = jnp.sum(square[...], axis=-1, keepdims=True) / channels - moved * moved
        scale = lax.rsqrt(jnp.maximum(spread, 0.0) + 1e-06)
        center[...] = center[...] + moved
        total[...] = jnp.broadcast_to(scale, total.shape)

        @pl.loop(0, count // LEAVE)
        def _(step):
            rows = pl.ds(pl.multiple_of(step * LEAVE, LEAVE), LEAVE)
            middle, scale = center[rows, :], total[rows, :]
            for lane in range(0, channels, LANES):
                lanes = pl.ds(lane, LANES)
                wide = mixed[rows, lanes].astype(jnp.float32)
                normed = (wide - middle) * scale * gain_ref[:, lanes] + bias_ref[:, lanes]
                mixed[rows, lanes] = (normed * jax.nn.sigmoid(normed)).astype(jnp.bfloat16)

    def level(k):
        return z if k == 0 else near(k)

    def near_u(block, k):
        @pl.loop(1, side)
        def _(du):
            arrived(block, level(k), lax.rem(u + du, side), v)

    def near_v(block, k):
        @pl.loop(1, side)
        def _(dv):
            arrived(block, level(k), u, lax.rem(v + dv, side))

    def far_v(block, k):
        @pl.loop(1, side)
        def _(du):
            @pl.loop(1, side)
            def _(dv):
                arrived(block, level(k), lax.rem(u + du, side), lax.rem(v + dv, side))

    def compute(block, k):
        if k == 0:
            pl.when(block == 0)(prepare)
            hand_over(many(block, pieces), block).wait_recv()

        steps = [
            (act, part, half)
            for part in range(parts)
            for act in (project, convolve)
            for half in range(2)
        ]
        for act, part, half in steps[k * len(steps) // tall : (k + 1) * len(steps) // tall]:
            act(block, part, half)

        if k == tall - 1:
            all_sent(block)

    sites = [(-order["own"], lambda block: send_own(block))]
    for k in range(1, tall):
        sites.append((order["along_z"][k - 1], lambda block, k=k: arrived(block, near(k), u, v)))
    for name, act in (("along_u", near_u), ("near_v", near_v), ("far_v", far_v)):
        for k in range(tall):
            sites.append((order[name][k], lambda block, k=k, act=act: act(block, k)))
    for k in range(tall):
        sites.append((order["late"] + k, lambda block, k=k: compute(block, k)))
    assert all(offset <= order["late"] for offset, _ in sites[:-tall])

    def round_of(number, carry):
        for j in range(tall):
            for offset, act in sites:
                if offset % tall != j:
                    continue
                block = number - offset // tall
                first = ahead if offset < 0 else 0

                @pl.when((block >= first) & (block < blocks))
                def _(block=block, act=act):
                    act(block)

        return carry

    rounds = blocks + (order["late"] + tall - 1) // tall
    lax.fori_loop(0, rounds, round_of, 0)
    finish()

    @pl.when(sp + 1 < sp_size)
    def _():
        tail.wait_send()
        docs_tail.wait_send()


def activated_product(
    rows, docs, value_weight, gate_weight, conv_weight, norm_gain, norm_bias
):
    side = lax.axis_size("dp") // 2
    tall = lax.axis_size("sp") // side
    count, width = rows.shape
    channels = value_weight.shape[1]
    order = plan(side, tall, channels)
    blocks = order["blocks"]
    pieces = tall * side * side
    return pl.pallas_call(
        functools.partial(fused_kernel, side, tall, order),
        out_shape=pltpu.VMEM((count, channels), jnp.bfloat16),
        in_specs=[pl.BlockSpec(memory_space=pl.ANY)] * 4
        + [pl.BlockSpec(memory_space=pltpu.VMEM)] * 3,
        out_specs=pl.BlockSpec(memory_space=pltpu.VMEM),
        scratch_shapes=[
            pltpu.VMEM((blocks, width, 2 * channels // blocks), jnp.bfloat16),
            pltpu.VMEM((HALO + count, width), jnp.bfloat16),
            pltpu.VMEM((1, LANES + count), jnp.int32),
            pltpu.VMEM((HALO, channels), jnp.float32),
            pltpu.VMEM((HALO // 8, HALO + count + SPARE, LANES), jnp.float32),
            pltpu.VMEM((HALO // 8 - 1, HALO + count + SPARE, LANES), jnp.float32),
            pltpu.VMEM((7, count + SPARE, LANES), jnp.float32),
            pltpu.VMEM((count, LANES), jnp.float32),
            pltpu.VMEM((count, LANES), jnp.float32),
            pltpu.VMEM((count, LANES), jnp.float32),
            pltpu.SemaphoreType.DMA((7, blocks)),
            pltpu.SemaphoreType.DMA((blocks, pieces)),
            pltpu.SemaphoreType.DMA((blocks,)),
            pltpu.SemaphoreType.DMA((blocks, 2 * channels // (blocks * LANES))),
            pltpu.SemaphoreType.DMA((2,)),
            pltpu.SemaphoreType.DMA((4,)),
        ],
        compiler_params=pltpu.CompilerParams(
            collective_id=0, has_side_effects=True, vmem_limit_bytes=56 * 1024 * 1024
        ),
    )(
        rows, docs, value_weight, gate_weight, conv_weight, norm_gain[None], norm_bias[None]
    )


def per_device(tokens, documents, value_weight, gate_weight, conv_weight, norm_gain, norm_bias):
    batch, count, width = tokens.shape
    channels = value_weight.shape[1]
    rows = tokens.reshape(batch * count, width)
    out = activated_product(
        rows, documents, value_weight, gate_weight, conv_weight, norm_gain, norm_bias
    )
    return out.reshape(batch, count, channels)


def solution(mesh):
    return jax.shard_map(
        per_device,
        mesh=mesh,
        in_specs=(
            P("dp", "sp", None),
            P("dp", "sp"),
            P(("sp", "dp"), None),
            P(("sp", "dp"), None),
            P(),
            P(),
            P(),
        ),
        out_specs=P("dp", "sp", None),
        check_vma=False,
    )
```

```python
import functools

import jax
import jax.numpy as jnp
from jax import lax
from jax.experimental import pallas as pl
from jax.experimental.pallas import tpu as pltpu
from jax.sharding import PartitionSpec as P

KERNEL = 31
HALO = 32
LANES = 128
TILE = 128
SPARE = 8
LEAVE = 32
MESH = pl.DeviceIdType.MESH


def plan(side, tall, channels):
    order = dict(blocks=channels // LANES, after=6, tall_first=((1, 4, 7, 10, 13), (0, 2, 7, 8, 11, 13)), own=47)
    if side == 2 and tall == 4:
        order.update(along_z=(0, 4, 7), along_u=(0, 7, 9, 10), near_v=(5, 11, 12, 12), far_v=(9, 13, 14, 14), late=16)
    else:
        order.update(
            own=tall,
            along_z=tuple(range(1, tall)),
            along_u=tuple(range(2, tall + 2)),
            near_v=tuple(range(6, tall + 6)),
            far_v=tuple(range(6, tall + 6)),
            late=6 + tall,
        )
    return order


def fused_kernel(
    side, tall, order, tok_hbm, docs_hbm, value_hbm, gate_hbm, conv_hbm, gain_hbm,
    bias_hbm, mixed, weights, tok, docs, conv_ref, gain_ref, bias_ref, leading, trailing, taps, shifted, far, near_by, center,
    total, square, send, recv, cross, own, begin, halo
):
    sp, dp = lax.axis_index("sp"), lax.axis_index("dp")
    sp_size = lax.axis_size("sp")
    core, y = lax.rem(dp, 2), lax.div(dp, 2)
    z, x = lax.div(sp, side), lax.rem(sp, side)
    flip = core == 1
    u, v = jnp.where(flip, y, x), jnp.where(flip, x, y)
    depth = value_hbm.shape[0]
    count = tok_hbm.shape[0]
    blocks = order["blocks"]
    channels = value_hbm.shape[1]
    span = count // 2
    other = {"sp": sp, "dp": y * 2 + (1 - core)}
    here = (z * side + x) * side + y

    pieces = tall * side * side

    def device(dz, du, dv):
        dx, dy = jnp.where(flip, dv, du), jnp.where(flip, du, dv)
        return {"sp": dz * side + dx, "dp": dy * 2 + core}

    def number(pz, pu, pv):
        px, py = jnp.where(flip, pv, pu), jnp.where(flip, pu, pv)
        return (pz * side + px) * side + py

    def piece(which, block, q):
        return weights.at[
            block, pl.ds(pl.multiple_of((q * 2 + which) * depth, depth), depth), :
        ]

    def link(kind, block, q, target):
        return pltpu.make_async_remote_copy(
            src_ref=piece(core, block, q),
            dst_ref=piece(core, block, q),
            send_sem=send.at[kind, block],
            recv_sem=recv.at[block, q],
            device_id=target,
            device_id_type=MESH,
        )

    def hand_over(rows, block):
        return pltpu.make_async_remote_copy(
            src_ref=rows,
            dst_ref=rows,
            send_sem=send.at[6, block],
            recv_sem=cross.at[block],
            device_id=other,
            device_id_type=MESH,
        )

    def many(block, amount):
        return weights.at[block, pl.ds(0, amount * depth), :]

    def tall_first(block):
        return functools.reduce(
            jnp.logical_or,
            [
                (core == which) & (block == chosen)
                for which in range(2)
                for chosen in order["tall_first"][which]
            ],
        )

    def spread(kind, block, q, at, source, extent, target, allowed):
        if source is at:
            if extent == 2:
                ways = (((None), 1 - at, kind),)
            else:
                ways = ((at + 1 < extent, at + 1, kind), (at > 0, at - 1, kind + 1))
        elif extent == 2:
            return
        else:
            rising = at > source
            onward = jnp.where(rising, at + 1, at - 1)
            inside = (onward >= 0) & (onward < extent)
            ways = ((inside, onward, jnp.where(rising, kind, kind + 1)),)
        for taken, onward, which in ways:
            conditions = [c for c in (taken, allowed) if c is not None]
            copy = link(which, block, q, target(onward))
            if conditions:
                pl.when(functools.reduce(jnp.logical_and, conditions))(copy.start)
            else:
                copy.start()

    def pass_on(block, pz, pu, pv):
        q = number(pz, pu, pv)
        first = tall_first(block)
        if pv is v:
            along_z = None if pu is u else jnp.logical_not(first)
            spread(0, block, q, z, pz, tall, lambda to: device(to, u, v), along_z)
            along_u = None if pz is z else first
            spread(2, block, q, u, pu, side, lambda to: device(z, to, v), along_u)
        spread(4, block, q, v, pv, side, lambda to: device(z, u, to), None)
        hand_over(piece(core, block, q), block).start()

    def sent(kind, block, amount, choices):
        for chosen in choices:
            copy = pltpu.make_async_remote_copy(
                src_ref=many(block, chosen),
                dst_ref=many(block, chosen),
                send_sem=send.at[kind, block],
                recv_sem=cross.at[block],
                device_id=other,
                device_id_type=MESH,
            )
            pl.when(amount == chosen)(copy.wait_send)

    def all_sent(block):
        first = tall_first(block)
        across = jnp.where(first, 1, side)
        up = jnp.where(z + 1 < tall, (z + 1) * across, 0)
        down = jnp.where(z > 0, (tall - z) * across, 0)
        choices = sorted({n * m for n in range(1, tall + 1) for m in (1, side)})
        sent(0, block, up, choices)
        sent(1, block, down, choices)
        height = jnp.where(first, tall, 1)
        if side == 2:
            sent(2, block, height, (1, tall))
        else:
            choices = sorted({n * m for n in range(1, side + 1) for m in (1, tall)})
            sent(2, block, jnp.where(u + 1 < side, (u + 1) * height, 0), choices)
            sent(3, block, jnp.where(u > 0, (side - u) * height, 0), choices)
        plane = tall * side
        if side == 2:
            sent(4, block, jnp.int32(plane), (plane,))
        else:
            choices = [n * plane for n in range(1, side + 1)]
            sent(4, block, jnp.where(v + 1 < side, (v + 1) * plane, 0), choices)
            sent(5, block, jnp.where(v > 0, (side - v) * plane, 0), choices)
        hand_over(many(block, pieces), block).wait_send()

    def arrived(block, pz, pu, pv):
        link(0, block, number(pz, pu, pv), other).wait_recv()
        pass_on(block, pz, pu, pv)

    low = jnp.minimum(z, tall - 1 - z)

    def near(k):
        step = jnp.where(lax.rem(k, 2) == 1, low - lax.div(k + 1, 2), low + lax.div(k, 2))
        at = jnp.where(k <= 2 * low, step, k)
        return jnp.where(z == low, at, tall - 1 - at)

    def own_copies(block):
        rows = pl.ds(pl.multiple_of((here * 2 + core) * depth, depth), depth)
        first = pl.multiple_of(block * LANES, LANES)
        for half, source in enumerate((value_hbm, gate_hbm)):
            yield pltpu.make_async_copy(
                source.at[:, pl.ds(first, LANES)],
                weights.at[block, rows, pl.ds(half * LANES, LANES)],
                own.at[block, half],
            )

    def send_own(block):
        for copy in own_copies(block):
            copy.wait()
        pass_on(block, z, u, v)

    barrier = pltpu.get_barrier_semaphore()
    greeted = jnp.int32(1)
    pl.semaphore_signal(barrier, inc=1, device_id=other, device_id_type=MESH)
    for there, target in (
        (z + 1 < tall, device(z + 1, u, v)),
        (z > 0, device(z - 1, u, v)),
        (u + 1 < side, device(z, u + 1, v)),
        (u > 0, device(z, u - 1, v)),
        (v + 1 < side, device(z, u, v + 1)),
        (v > 0, device(z, u, v - 1)),
        (sp + 1 < sp_size, {"sp": sp + 1, "dp": dp}),
        (sp > 0, {"sp": sp - 1, "dp": dp}),
    ):
        greeted = greeted + there.astype(jnp.int32)

        @pl.when(there)
        def _(target=target):
            pl.semaphore_signal(barrier, inc=1, device_id=target, device_id_type=MESH)

    @pl.loop(0, blocks)
    def _(block):
        for copy in own_copies(block):
            copy.start()

    load = pltpu.make_async_copy(tok_hbm, tok, begin.at[0])
    load.start()
    read = pltpu.make_async_copy(docs_hbm, docs.at[:, pl.ds(LANES, count)], begin.at[1])
    read.start()
    small = [
        pltpu.make_async_copy(source, target, begin.at[2 + i])
        for i, (source, target) in enumerate(
            ((conv_hbm, conv_ref), (gain_hbm, gain_ref), (bias_hbm, bias_ref))
        )
    ]
    for copy in small:
        copy.start()

    pl.semaphore_wait(barrier, greeted)

    following = {"sp": lax.rem(sp + 1, sp_size), "dp": dp}
    def tail(block):
        return pltpu.make_async_remote_copy(
            src_ref=trailing.at[block],
            dst_ref=leading.at[block],
            send_sem=halo.at[0, block],
            recv_sem=halo.at[1, block],
            device_id=following,
            device_id_type=MESH,
        )

    docs_tail = pltpu.make_async_remote_copy(
        src_ref=docs_hbm.at[:, pl.ds(count - LANES, LANES)],
        dst_ref=docs.at[:, pl.ds(0, LANES)],
        send_sem=halo.at[0, blocks],
        recv_sem=halo.at[1, blocks],
        device_id=following,
        device_id_type=MESH,
    )

    @pl.when(sp + 1 < sp_size)
    def _():
        docs_tail.start()

    ahead = min(blocks, -(-order["own"] // tall))

    @pl.loop(0, ahead)
    def _(block):
        send_own(block)

    @pl.when(sp == 0)
    def _():
        leading[...] = jnp.zeros_like(leading)
        docs[:, pl.ds(0, LANES)] = jnp.full((1, LANES), -1, jnp.int32)

    def prepare():
        load.wait()
        read.wait()
        for copy in small:
            copy.wait()
        taps[pl.ds(0, KERNEL), :] = conv_ref[...].astype(jnp.float32)

        @pl.when(sp > 0)
        def _():
            docs_tail.wait_recv()

        column = jnp.broadcast_to(docs[...], (LANES, LANES + count)).T
        wide = column[LANES - HALO :]
        for lag in range(8, HALO, 8):
            same = wide[HALO - 8 :] == wide[HALO - 8 - lag : HALO + count - lag]
            far[lag // 8 - 1, pl.ds(HALO - 8, count + 8), :] = same.astype(jnp.float32)
        for lag in range(1, 8):
            same = wide[HALO:] == wide[HALO - lag : HALO + count - lag]
            near_by[lag - 1, pl.ds(0, count), :] = same.astype(jnp.float32)

        total[...] = jnp.zeros_like(total)
        square[...] = jnp.zeros_like(square)

    def project(block, half):
        rows = pl.ds(half * span, span)
        both = jnp.dot(tok[rows, :], weights[block], preferred_element_type=jnp.float32)
        value = both[:, :LANES].astype(jnp.bfloat16).astype(jnp.float32)
        gate = both[:, LANES:].astype(jnp.bfloat16).astype(jnp.float32)
        glu = (value * jax.nn.sigmoid(gate)).astype(jnp.bfloat16)
        base = lax.rem(block, 2) * (HALO // 8)
        shifted[base, pl.ds(HALO + half * span, span), :] = glu.astype(jnp.float32)
        if half:
            trailing[block] = glu[span - HALO :]

    def exchange(block):
        @pl.when(sp + 1 < sp_size)
        def _():
            tail(block).start()

    def convolve(block, half):
        lanes = pl.ds(pl.multiple_of(block * LANES, LANES), LANES)
        base = lax.rem(block, 2) * (HALO // 8)
        if half == 0:
            @pl.when(sp > 0)
            def _():
                tail(block).wait_recv()

            shifted[base, pl.ds(0, HALO), :] = leading[block].astype(jnp.float32)
        start = half * span + HALO - 8
        kept = pl.ds(start, span + 8)
        for a in range(1, HALO // 8):
            moved = shifted[base, pl.ds(start - 8 * a, span + 8), :]
            shifted[base + a, kept, :] = moved * far[a - 1, kept, :]

        @pl.loop(0, span // TILE)
        def _(tile):
            top = pl.multiple_of(half * span + tile * TILE, TILE)
            held = None
            for r in range(8):
                run = None
                for a in range(HALO // 8):
                    lag = 8 * a + r
                    if lag < KERNEL:
                        moved = shifted[base + a, pl.ds(top + HALO - r, TILE), :]
                        term = moved * taps[lag : lag + 1, lanes]
                        run = term if run is None else run + term
                if r:
                    run = run * near_by[r - 1, pl.ds(top, TILE), :]
                held = run if held is None else held + run
            rows = pl.ds(top, TILE)
            rounded = held.astype(jnp.bfloat16)
            mixed[rows, lanes] = rounded
            held = rounded.astype(jnp.float32)

            @pl.when(block == 0)
            def _():
                middle = jnp.mean(held, axis=-1, keepdims=True)
                center[rows, :] = jnp.broadcast_to(middle, (TILE, LANES))

            off = held - center[rows, :]
            total[rows, :] += off
            square[rows, :] += off * off

    def finish():
        moved = jnp.sum(total[...], axis=-1, keepdims=True) / channels
        spread = jnp.sum(square[...], axis=-1, keepdims=True) / channels - moved * moved
        scale = lax.rsqrt(jnp.maximum(spread, 0.0) + 1e-06)
        center[...] = center[...] + moved
        total[...] = jnp.broadcast_to(scale, total.shape)

        @pl.loop(0, count // LEAVE)
        def _(step):
            rows = pl.ds(pl.multiple_of(step * LEAVE, LEAVE), LEAVE)
            middle, scale = center[rows, :], total[rows, :]
            for lane in range(0, channels, LANES):
                lanes = pl.ds(lane, LANES)
                wide = mixed[rows, lanes].astype(jnp.float32)
                normed = (wide - middle) * scale * gain_ref[:, lanes] + bias_ref[:, lanes]
                mixed[rows, lanes] = (normed * jax.nn.sigmoid(normed)).astype(jnp.bfloat16)

    def level(k):
        return z if k == 0 else near(k)

    def near_u(block, k):
        @pl.loop(1, side)
        def _(du):
            arrived(block, level(k), lax.rem(u + du, side), v)

    def near_v(block, k):
        @pl.loop(1, side)
        def _(dv):
            arrived(block, level(k), u, lax.rem(v + dv, side))

    def far_v(block, k):
        @pl.loop(1, side)
        def _(du):
            @pl.loop(1, side)
            def _(dv):
                arrived(block, level(k), lax.rem(u + du, side), lax.rem(v + dv, side))

    def compute(block, k):
        if k == 0:
            pl.when(block == 0)(prepare)
            hand_over(many(block, pieces), block).wait_recv()

            project(block, 1)
        if k == 1:
            exchange(block)
            project(block, 0)
        if k == tall - 1:
            all_sent(block)

    sites = [(-order["own"], lambda block: send_own(block))]
    for k in range(1, tall):
        sites.append((order["along_z"][k - 1], lambda block, k=k: arrived(block, near(k), u, v)))
    for name, act in (("along_u", near_u), ("near_v", near_v), ("far_v", far_v)):
        for k in range(tall):
            sites.append((order[name][k], lambda block, k=k, act=act: act(block, k)))
    assert all(offset <= order["late"] for offset, _ in sites)
    for k in range(tall):
        sites.append((order["late"] + k, lambda block, k=k: compute(block, k)))
    for half in range(2):
        place = order["late"] + order["after"] + 1 - half
        sites.append((place, lambda block, half=half: convolve(block, half)))

    def round_of(number, carry):
        for j in range(tall):
            for offset, act in sites:
                if offset % tall != j:
                    continue
                block = number - offset // tall
                first = ahead if offset < 0 else 0

                @pl.when((block >= first) & (block < blocks))
                def _(block=block, act=act):
                    act(block)

        return carry

    rounds = blocks + (order["late"] + order["after"] + tall) // tall
    lax.fori_loop(0, rounds, round_of, 0)
    finish()

    @pl.when(sp + 1 < sp_size)
    def _():
        @pl.loop(0, blocks)
        def _(block):
            tail(block).wait_send()

        docs_tail.wait_send()


def activated_product(
    rows, docs, value_weight, gate_weight, conv_weight, norm_gain, norm_bias
):
    side = lax.axis_size("dp") // 2
    tall = lax.axis_size("sp") // side
    count, width = rows.shape
    channels = value_weight.shape[1]
    order = plan(side, tall, channels)
    blocks = order["blocks"]
    pieces = tall * side * side
    return pl.pallas_call(
        functools.partial(fused_kernel, side, tall, order),
        out_shape=pltpu.VMEM((count, channels), jnp.bfloat16),
        in_specs=[pl.BlockSpec(memory_space=pl.ANY)] * 7,
        out_specs=pl.BlockSpec(memory_space=pltpu.VMEM),
        scratch_shapes=[
            pltpu.VMEM((blocks, width, 2 * channels // blocks), jnp.bfloat16),
            pltpu.VMEM((count, width), jnp.bfloat16),
            pltpu.VMEM((1, LANES + count), jnp.int32),
            pltpu.VMEM(conv_weight.shape, conv_weight.dtype),
            pltpu.VMEM((1, channels), jnp.float32),
            pltpu.VMEM((1, channels), jnp.float32),
            pltpu.VMEM((blocks, HALO, LANES), jnp.bfloat16),
            pltpu.VMEM((blocks, HALO, LANES), jnp.bfloat16),
            pltpu.VMEM((HALO, channels), jnp.float32),
            pltpu.VMEM((2 * (HALO // 8), HALO + count + SPARE, LANES), jnp.float32),
            pltpu.VMEM((HALO // 8 - 1, HALO + count + SPARE, LANES), jnp.float32),
            pltpu.VMEM((7, count + SPARE, LANES), jnp.float32),
            pltpu.VMEM((count, LANES), jnp.float32),
            pltpu.VMEM((count, LANES), jnp.float32),
            pltpu.VMEM((count, LANES), jnp.float32),
            pltpu.SemaphoreType.DMA((7, blocks)),
            pltpu.SemaphoreType.DMA((blocks, pieces)),
            pltpu.SemaphoreType.DMA((blocks,)),
            pltpu.SemaphoreType.DMA((blocks, 2)),
            pltpu.SemaphoreType.DMA((5,)),
            pltpu.SemaphoreType.DMA((2, blocks + 1)),
        ],
        compiler_params=pltpu.CompilerParams(
            collective_id=0, has_side_effects=True, vmem_limit_bytes=56 * 1024 * 1024
        ),
    )(
        rows, docs, value_weight, gate_weight, conv_weight, norm_gain[None], norm_bias[None]
    )


def per_device(tokens, documents, value_weight, gate_weight, conv_weight, norm_gain, norm_bias):
    batch, count, width = tokens.shape
    channels = value_weight.shape[1]
    rows = tokens.reshape(batch * count, width)
    out = activated_product(
        rows, documents, value_weight, gate_weight, conv_weight, norm_gain, norm_bias
    )
    return out.reshape(batch, count, channels)


def solution(mesh):
    return jax.shard_map(
        per_device,
        mesh=mesh,
        in_specs=(
            P("dp", "sp", None),
            P("dp", "sp"),
            P(("sp", "dp"), None),
            P(("sp", "dp"), None),
            P(),
            P(),
            P(),
        ),
        out_specs=P("dp", "sp", None),
        check_vma=False,
    )
```

```python
import functools

import jax
import jax.numpy as jnp
from jax import lax
from jax.experimental import pallas as pl
from jax.experimental.pallas import tpu as pltpu
from jax.sharding import PartitionSpec as P

KERNEL = 31
HALO = 32
LANES = 128
TILE = 128
SPARE = 8
LEAVE = 32
MESH = pl.DeviceIdType.MESH


def plan(side, tall, channels):
    order = dict(blocks=channels // LANES, after=6, tall_first=((1, 4, 5, 10, 13), (1, 2, 7, 8, 11, 13)), own=34)
    if side == 2 and tall == 4:
        order.update(along_z=(0, 4, 7), along_u=(0, 7, 7, 10), near_v=(7, 9, 11, 13), far_v=(7, 15, 16, 16), late=17)
    else:
        order.update(
            own=tall,
            along_z=tuple(range(1, tall)),
            along_u=tuple(range(2, tall + 2)),
            near_v=tuple(range(6, tall + 6)),
            far_v=tuple(range(6, tall + 6)),
            late=6 + tall,
        )
    return order


def fused_kernel(
    side, tall, order, tok_hbm, docs_hbm, value_hbm, gate_hbm, conv_hbm, gain_hbm,
    bias_hbm, mixed, weights, tok, docs, conv_ref, gain_ref, bias_ref, leading, trailing, taps, shifted, far, near_by, center,
    total, square, send, recv, cross, own, begin, halo
):
    sp, dp = lax.axis_index("sp"), lax.axis_index("dp")
    sp_size = lax.axis_size("sp")
    core, y = lax.rem(dp, 2), lax.div(dp, 2)
    z, x = lax.div(sp, side), lax.rem(sp, side)
    flip = core == 1
    u, v = jnp.where(flip, y, x), jnp.where(flip, x, y)
    depth = value_hbm.shape[0]
    count = tok_hbm.shape[0]
    blocks = order["blocks"]
    channels = value_hbm.shape[1]
    span = count // 2
    slots = shifted.shape[0] // (HALO // 8)
    other = {"sp": sp, "dp": y * 2 + (1 - core)}
    here = (z * side + x) * side + y

    pieces = tall * side * side

    def device(dz, du, dv):
        dx, dy = jnp.where(flip, dv, du), jnp.where(flip, du, dv)
        return {"sp": dz * side + dx, "dp": dy * 2 + core}

    def number(pz, pu, pv):
        px, py = jnp.where(flip, pv, pu), jnp.where(flip, pu, pv)
        return (pz * side + px) * side + py

    def piece(which, block, q):
        return weights.at[
            block, pl.ds(pl.multiple_of((q * 2 + which) * depth, depth), depth), :
        ]

    def link(kind, block, q, target):
        return pltpu.make_async_remote_copy(
            src_ref=piece(core, block, q),
            dst_ref=piece(core, block, q),
            send_sem=send.at[kind, block],
            recv_sem=recv.at[block, q],
            device_id=target,
            device_id_type=MESH,
        )

    def hand_over(rows, block):
        return pltpu.make_async_remote_copy(
            src_ref=rows,
            dst_ref=rows,
            send_sem=send.at[6, block],
            recv_sem=cross.at[block],
            device_id=other,
            device_id_type=MESH,
        )

    def many(block, amount):
        return weights.at[block, pl.ds(0, amount * depth), :]

    def tall_first(block):
        return functools.reduce(
            jnp.logical_or,
            [
                (core == which) & (block == chosen)
                for which in range(2)
                for chosen in order["tall_first"][which]
            ],
        )

    def spread(kind, block, q, at, source, extent, target, allowed):
        if source is at:
            if extent == 2:
                ways = (((None), 1 - at, kind),)
            else:
                ways = ((at + 1 < extent, at + 1, kind), (at > 0, at - 1, kind + 1))
        elif extent == 2:
            return
        else:
            rising = at > source
            onward = jnp.where(rising, at + 1, at - 1)
            inside = (onward >= 0) & (onward < extent)
            ways = ((inside, onward, jnp.where(rising, kind, kind + 1)),)
        for taken, onward, which in ways:
            conditions = [c for c in (taken, allowed) if c is not None]
            copy = link(which, block, q, target(onward))
            if conditions:
                pl.when(functools.reduce(jnp.logical_and, conditions))(copy.start)
            else:
                copy.start()

    def pass_on(block, pz, pu, pv):
        q = number(pz, pu, pv)
        first = tall_first(block)
        if pv is v:
            along_z = None if pu is u else jnp.logical_not(first)
            spread(0, block, q, z, pz, tall, lambda to: device(to, u, v), along_z)
            along_u = None if pz is z else first
            spread(2, block, q, u, pu, side, lambda to: device(z, to, v), along_u)
        spread(4, block, q, v, pv, side, lambda to: device(z, u, to), None)
        hand_over(piece(core, block, q), block).start()

    def sent(kind, block, amount, choices):
        for chosen in choices:
            copy = pltpu.make_async_remote_copy(
                src_ref=many(block, chosen),
                dst_ref=many(block, chosen),
                send_sem=send.at[kind, block],
                recv_sem=cross.at[block],
                device_id=other,
                device_id_type=MESH,
            )
            pl.when(amount == chosen)(copy.wait_send)

    def all_sent(block):
        first = tall_first(block)
        across = jnp.where(first, 1, side)
        up = jnp.where(z + 1 < tall, (z + 1) * across, 0)
        down = jnp.where(z > 0, (tall - z) * across, 0)
        choices = sorted({n * m for n in range(1, tall + 1) for m in (1, side)})
        sent(0, block, up, choices)
        sent(1, block, down, choices)
        height = jnp.where(first, tall, 1)
        if side == 2:
            sent(2, block, height, (1, tall))
        else:
            choices = sorted({n * m for n in range(1, side + 1) for m in (1, tall)})
            sent(2, block, jnp.where(u + 1 < side, (u + 1) * height, 0), choices)
            sent(3, block, jnp.where(u > 0, (side - u) * height, 0), choices)
        plane = tall * side
        if side == 2:
            sent(4, block, jnp.int32(plane), (plane,))
        else:
            choices = [n * plane for n in range(1, side + 1)]
            sent(4, block, jnp.where(v + 1 < side, (v + 1) * plane, 0), choices)
            sent(5, block, jnp.where(v > 0, (side - v) * plane, 0), choices)
        hand_over(many(block, pieces), block).wait_send()

    def arrived(block, pz, pu, pv):
        link(0, block, number(pz, pu, pv), other).wait_recv()
        pass_on(block, pz, pu, pv)

    low = jnp.minimum(z, tall - 1 - z)

    def near(k):
        step = jnp.where(lax.rem(k, 2) == 1, low - lax.div(k + 1, 2), low + lax.div(k, 2))
        at = jnp.where(k <= 2 * low, step, k)
        return jnp.where(z == low, at, tall - 1 - at)

    def own_copies(block):
        rows = pl.ds(pl.multiple_of((here * 2 + core) * depth, depth), depth)
        first = pl.multiple_of(block * LANES, LANES)
        for half, source in enumerate((value_hbm, gate_hbm)):
            yield pltpu.make_async_copy(
                source.at[:, pl.ds(first, LANES)],
                weights.at[block, rows, pl.ds(half * LANES, LANES)],
                own.at[block, half],
            )

    def send_own(block):
        for copy in own_copies(block):
            copy.wait()
        pass_on(block, z, u, v)

    barrier = pltpu.get_barrier_semaphore()
    greeted = jnp.int32(1)
    pl.semaphore_signal(barrier, inc=1, device_id=other, device_id_type=MESH)
    for there, target in (
        (z + 1 < tall, device(z + 1, u, v)),
        (z > 0, device(z - 1, u, v)),
        (u + 1 < side, device(z, u + 1, v)),
        (u > 0, device(z, u - 1, v)),
        (v + 1 < side, device(z, u, v + 1)),
        (v > 0, device(z, u, v - 1)),
        (sp + 1 < sp_size, {"sp": sp + 1, "dp": dp}),
        (sp > 0, {"sp": sp - 1, "dp": dp}),
    ):
        greeted = greeted + there.astype(jnp.int32)

        @pl.when(there)
        def _(target=target):
            pl.semaphore_signal(barrier, inc=1, device_id=target, device_id_type=MESH)

    @pl.loop(0, blocks)
    def _(block):
        for copy in own_copies(block):
            copy.start()

    load = pltpu.make_async_copy(tok_hbm, tok, begin.at[0])
    load.start()
    read = pltpu.make_async_copy(docs_hbm, docs.at[:, pl.ds(LANES, count)], begin.at[1])
    read.start()
    small = [
        pltpu.make_async_copy(source, target, begin.at[2 + i])
        for i, (source, target) in enumerate(
            ((conv_hbm, conv_ref), (gain_hbm, gain_ref), (bias_hbm, bias_ref))
        )
    ]
    for copy in small:
        copy.start()

    pl.semaphore_wait(barrier, greeted)

    following = {"sp": lax.rem(sp + 1, sp_size), "dp": dp}
    def tail(block):
        return pltpu.make_async_remote_copy(
            src_ref=trailing.at[block],
            dst_ref=leading.at[block],
            send_sem=halo.at[0, block],
            recv_sem=halo.at[1, block],
            device_id=following,
            device_id_type=MESH,
        )

    docs_tail = pltpu.make_async_remote_copy(
        src_ref=docs_hbm.at[:, pl.ds(count - LANES, LANES)],
        dst_ref=docs.at[:, pl.ds(0, LANES)],
        send_sem=halo.at[0, blocks],
        recv_sem=halo.at[1, blocks],
        device_id=following,
        device_id_type=MESH,
    )

    @pl.when(sp + 1 < sp_size)
    def _():
        docs_tail.start()

    ahead = min(blocks, -(-order["own"] // tall))

    @pl.loop(0, ahead)
    def _(block):
        send_own(block)

    @pl.when(sp == 0)
    def _():
        leading[...] = jnp.zeros_like(leading)
        docs[:, pl.ds(0, LANES)] = jnp.full((1, LANES), -1, jnp.int32)

    def prepare():
        load.wait()
        read.wait()
        for copy in small:
            copy.wait()
        taps[pl.ds(0, KERNEL), :] = conv_ref[...].astype(jnp.float32)

        @pl.when(sp > 0)
        def _():
            docs_tail.wait_recv()

        column = jnp.broadcast_to(docs[...], (LANES, LANES + count)).T
        wide = column[LANES - HALO :]
        for lag in range(8, HALO, 8):
            same = wide[HALO - 8 :] == wide[HALO - 8 - lag : HALO + count - lag]
            far[lag // 8 - 1, pl.ds(HALO - 8, count + 8), :] = same.astype(jnp.float32)
        for lag in range(1, 8):
            same = wide[HALO:] == wide[HALO - lag : HALO + count - lag]
            near_by[lag - 1, pl.ds(0, count), :] = same.astype(jnp.float32)

        total[...] = jnp.zeros_like(total)
        square[...] = jnp.zeros_like(square)

    def project(block, half):
        rows = pl.ds(half * span, span)
        both = jnp.dot(tok[rows, :], weights[block], preferred_element_type=jnp.float32)
        value = both[:, :LANES].astype(jnp.bfloat16).astype(jnp.float32)
        gate = both[:, LANES:].astype(jnp.bfloat16).astype(jnp.float32)
        glu = (value * jax.nn.sigmoid(gate)).astype(jnp.bfloat16)
        base = lax.rem(block, slots) * (HALO // 8)
        shifted[base, pl.ds(HALO + half * span, span), :] = glu.astype(jnp.float32)
        if half:
            trailing[block] = glu[span - HALO :]

    def exchange(block):
        @pl.when(sp + 1 < sp_size)
        def _():
            tail(block).start()

    def convolve(block, half):
        lanes = pl.ds(pl.multiple_of(block * LANES, LANES), LANES)
        base = lax.rem(block, slots) * (HALO // 8)
        if half == 0:
            @pl.when(sp > 0)
            def _():
                tail(block).wait_recv()

            shifted[base, pl.ds(0, HALO), :] = leading[block].astype(jnp.float32)
        start = half * span + HALO - 8
        kept = pl.ds(start, span + 8)
        for a in range(1, HALO // 8):
            moved = shifted[base, pl.ds(start - 8 * a, span + 8), :]
            shifted[base + a, kept, :] = moved * far[a - 1, kept, :]

        @pl.loop(0, span // TILE)
        def _(tile):
            top = pl.multiple_of(half * span + tile * TILE, TILE)
            held = None
            for r in range(8):
                run = None
                for a in range(HALO // 8):
                    lag = 8 * a + r
                    if lag < KERNEL:
                        moved = shifted[base + a, pl.ds(top + HALO - r, TILE), :]
                        term = moved * taps[lag : lag + 1, lanes]
                        run = term if run is None else run + term
                if r:
                    run = run * near_by[r - 1, pl.ds(top, TILE), :]
                held = run if held is None else held + run
            rows = pl.ds(top, TILE)
            rounded = held.astype(jnp.bfloat16)
            mixed[rows, lanes] = rounded
            held = rounded.astype(jnp.float32)

            @pl.when(block == 0)
            def _():
                middle = jnp.mean(held, axis=-1, keepdims=True)
                center[rows, :] = jnp.broadcast_to(middle, (TILE, LANES))

            off = held - center[rows, :]
            total[rows, :] += off
            square[rows, :] += off * off

    def finish():
        moved = jnp.sum(total[...], axis=-1, keepdims=True) / channels
        spread = jnp.sum(square[...], axis=-1, keepdims=True) / channels - moved * moved
        scale = lax.rsqrt(jnp.maximum(spread, 0.0) + 1e-06)
        center[...] = center[...] + moved
        total[...] = jnp.broadcast_to(scale, total.shape)

        @pl.loop(0, count // LEAVE)
        def _(step):
            rows = pl.ds(pl.multiple_of(step * LEAVE, LEAVE), LEAVE)
            middle, scale = center[rows, :], total[rows, :]
            for lane in range(0, channels, LANES):
                lanes = pl.ds(lane, LANES)
                wide = mixed[rows, lanes].astype(jnp.float32)
                normed = (wide - middle) * scale * gain_ref[:, lanes] + bias_ref[:, lanes]
                mixed[rows, lanes] = (normed * jax.nn.sigmoid(normed)).astype(jnp.bfloat16)

    def level(k):
        return z if k == 0 else near(k)

    def near_u(block, k):
        @pl.loop(1, side)
        def _(du):
            arrived(block, level(k), lax.rem(u + du, side), v)

    def near_v(block, k):
        @pl.loop(1, side)
        def _(dv):
            arrived(block, level(k), u, lax.rem(v + dv, side))

    def far_v(block, k):
        @pl.loop(1, side)
        def _(du):
            @pl.loop(1, side)
            def _(dv):
                arrived(block, level(k), lax.rem(u + du, side), lax.rem(v + dv, side))

    def compute(block, k):
        if k == 0:
            pl.when(block == 0)(prepare)
            hand_over(many(block, pieces), block).wait_recv()

            project(block, 1)
        if k == 1:
            exchange(block)
            project(block, 0)
        if k == tall - 1:
            all_sent(block)

    sites = [(-order["own"], lambda block: send_own(block))]
    for k in range(1, tall):
        sites.append((order["along_z"][k - 1], lambda block, k=k: arrived(block, near(k), u, v)))
    for name, act in (("along_u", near_u), ("near_v", near_v), ("far_v", far_v)):
        for k in range(tall):
            sites.append((order[name][k], lambda block, k=k, act=act: act(block, k)))
    assert all(offset <= order["late"] for offset, _ in sites)
    for k in range(tall):
        sites.append((order["late"] + k, lambda block, k=k: compute(block, k)))
    for half in range(2):
        place = order["late"] + order["after"] + 1 - half
        sites.append((place, lambda block, half=half: convolve(block, half)))

    def round_of(number, carry):
        for j in range(tall):
            for offset, act in sites:
                if offset % tall != j:
                    continue
                block = number - offset // tall
                first = ahead if offset < 0 else 0

                @pl.when((block >= first) & (block < blocks))
                def _(block=block, act=act):
                    act(block)

        return carry

    rounds = blocks + (order["late"] + order["after"] + tall) // tall
    lax.fori_loop(0, rounds, round_of, 0)
    finish()

    @pl.when(sp + 1 < sp_size)
    def _():
        @pl.loop(0, blocks)
        def _(block):
            tail(block).wait_send()

        docs_tail.wait_send()


def activated_product(
    rows, docs, value_weight, gate_weight, conv_weight, norm_gain, norm_bias
):
    side = lax.axis_size("dp") // 2
    tall = lax.axis_size("sp") // side
    count, width = rows.shape
    channels = value_weight.shape[1]
    order = plan(side, tall, channels)
    blocks = order["blocks"]
    slots = (order["after"] + 1) // tall + 1
    pieces = tall * side * side
    return pl.pallas_call(
        functools.partial(fused_kernel, side, tall, order),
        out_shape=pltpu.VMEM((count, channels), jnp.bfloat16),
        in_specs=[pl.BlockSpec(memory_space=pl.ANY)] * 7,
        out_specs=pl.BlockSpec(memory_space=pltpu.VMEM),
        scratch_shapes=[
            pltpu.VMEM((blocks, width, 2 * channels // blocks), jnp.bfloat16),
            pltpu.VMEM((count, width), jnp.bfloat16),
            pltpu.VMEM((1, LANES + count), jnp.int32),
            pltpu.VMEM(conv_weight.shape, conv_weight.dtype),
            pltpu.VMEM((1, channels), jnp.float32),
            pltpu.VMEM((1, channels), jnp.float32),
            pltpu.VMEM((blocks, HALO, LANES), jnp.bfloat16),
            pltpu.VMEM((blocks, HALO, LANES), jnp.bfloat16),
            pltpu.VMEM((HALO, channels), jnp.float32),
            pltpu.VMEM((slots * (HALO // 8), HALO + count + SPARE, LANES), jnp.float32),
            pltpu.VMEM((HALO // 8 - 1, HALO + count + SPARE, LANES), jnp.float32),
            pltpu.VMEM((7, count + SPARE, LANES), jnp.float32),
            pltpu.VMEM((count, LANES), jnp.float32),
            pltpu.VMEM((count, LANES), jnp.float32),
            pltpu.VMEM((count, LANES), jnp.float32),
            pltpu.SemaphoreType.DMA((7, blocks)),
            pltpu.SemaphoreType.DMA((blocks, pieces)),
            pltpu.SemaphoreType.DMA((blocks,)),
            pltpu.SemaphoreType.DMA((blocks, 2)),
            pltpu.SemaphoreType.DMA((5,)),
            pltpu.SemaphoreType.DMA((2, blocks + 1)),
        ],
        compiler_params=pltpu.CompilerParams(
            collective_id=0, has_side_effects=True, vmem_limit_bytes=56 * 1024 * 1024
        ),
    )(
        rows, docs, value_weight, gate_weight, conv_weight, norm_gain[None], norm_bias[None]
    )


def per_device(tokens, documents, value_weight, gate_weight, conv_weight, norm_gain, norm_bias):
    batch, count, width = tokens.shape
    channels = value_weight.shape[1]
    rows = tokens.reshape(batch * count, width)
    out = activated_product(
        rows, documents, value_weight, gate_weight, conv_weight, norm_gain, norm_bias
    )
    return out.reshape(batch, count, channels)


def solution(mesh):
    return jax.shard_map(
        per_device,
        mesh=mesh,
        in_specs=(
            P("dp", "sp", None),
            P("dp", "sp"),
            P(("sp", "dp"), None),
            P(("sp", "dp"), None),
            P(),
            P(),
            P(),
        ),
        out_specs=P("dp", "sp", None),
        check_vma=False,
    )
```

```python
import functools

import jax
import jax.numpy as jnp
from jax import lax
from jax.experimental import pallas as pl
from jax.experimental.pallas import tpu as pltpu
from jax.sharding import PartitionSpec as P

KERNEL = 31
HALO = 32
LANES = 128
TILE = 128
SPARE = 8
LEAVE = 32
MESH = pl.DeviceIdType.MESH


def plan(side, tall, channels):
    order = dict(blocks=channels // LANES, after=6, tall_first=((1, 4, 5, 10, 13), (1, 2, 7, 8, 11, 13)), own=34)
    if side == 2 and tall == 4:
        order.update(along_z=(0, 4, 7), along_u=(0, 7, 7, 10), near_v=(7, 9, 11, 13), far_v=(7, 15, 16, 16), late=17)
    else:
        order.update(
            own=tall,
            along_z=tuple(range(1, tall)),
            along_u=tuple(range(2, tall + 2)),
            near_v=tuple(range(6, tall + 6)),
            far_v=tuple(range(6, tall + 6)),
            late=6 + tall,
        )
    return order


def fused_kernel(
    side, tall, order, tok_hbm, docs_hbm, value_hbm, gate_hbm, conv_hbm, gain_hbm,
    bias_hbm, mixed, weights, tok, docs, conv_ref, gain_ref, bias_ref, leading, trailing, taps, shifted, far, near_by, center,
    total, square, send, recv, cross, own, begin, halo
):
    sp, dp = lax.axis_index("sp"), lax.axis_index("dp")
    sp_size = lax.axis_size("sp")
    core, y = lax.rem(dp, 2), lax.div(dp, 2)
    z, x = lax.div(sp, side), lax.rem(sp, side)
    flip = core == 1
    u, v = jnp.where(flip, y, x), jnp.where(flip, x, y)
    depth = value_hbm.shape[0]
    count = tok_hbm.shape[0]
    blocks = order["blocks"]
    channels = value_hbm.shape[1]
    span = count // 2
    slots = shifted.shape[0] // (HALO // 8)
    other = {"sp": sp, "dp": y * 2 + (1 - core)}
    here = (z * side + x) * side + y

    pieces = tall * side * side

    def device(dz, du, dv):
        dx, dy = jnp.where(flip, dv, du), jnp.where(flip, du, dv)
        return {"sp": dz * side + dx, "dp": dy * 2 + core}

    def number(pz, pu, pv):
        px, py = jnp.where(flip, pv, pu), jnp.where(flip, pu, pv)
        return (pz * side + px) * side + py

    def piece(which, block, q):
        return weights.at[
            block, pl.ds(pl.multiple_of((q * 2 + which) * depth, depth), depth), :
        ]

    def link(kind, block, q, target):
        return pltpu.make_async_remote_copy(
            src_ref=piece(core, block, q),
            dst_ref=piece(core, block, q),
            send_sem=send.at[kind, block],
            recv_sem=recv.at[block, q],
            device_id=target,
            device_id_type=MESH,
        )

    def hand_over(rows, block):
        return pltpu.make_async_remote_copy(
            src_ref=rows,
            dst_ref=rows,
            send_sem=send.at[6, block],
            recv_sem=cross.at[block],
            device_id=other,
            device_id_type=MESH,
        )

    def many(block, amount):
        return weights.at[block, pl.ds(0, amount * depth), :]

    def tall_first(block):
        return functools.reduce(
            jnp.logical_or,
            [
                (core == which) & (block == chosen)
                for which in range(2)
                for chosen in order["tall_first"][which]
            ],
        )

    def spread(kind, block, q, at, source, extent, target, allowed):
        if source is at:
            if extent == 2:
                ways = (((None), 1 - at, kind),)
            else:
                ways = ((at + 1 < extent, at + 1, kind), (at > 0, at - 1, kind + 1))
        elif extent == 2:
            return
        else:
            rising = at > source
            onward = jnp.where(rising, at + 1, at - 1)
            inside = (onward >= 0) & (onward < extent)
            ways = ((inside, onward, jnp.where(rising, kind, kind + 1)),)
        for taken, onward, which in ways:
            conditions = [c for c in (taken, allowed) if c is not None]
            copy = link(which, block, q, target(onward))
            if conditions:
                pl.when(functools.reduce(jnp.logical_and, conditions))(copy.start)
            else:
                copy.start()

    def pass_on(block, pz, pu, pv):
        q = number(pz, pu, pv)
        first = tall_first(block)
        if pv is v:
            along_z = None if pu is u else jnp.logical_not(first)
            spread(0, block, q, z, pz, tall, lambda to: device(to, u, v), along_z)
            along_u = None if pz is z else first
            spread(2, block, q, u, pu, side, lambda to: device(z, to, v), along_u)
        spread(4, block, q, v, pv, side, lambda to: device(z, u, to), None)
        hand_over(piece(core, block, q), block).start()

    def sent(kind, block, amount, choices):
        for chosen in choices:
            copy = pltpu.make_async_remote_copy(
                src_ref=many(block, chosen),
                dst_ref=many(block, chosen),
                send_sem=send.at[kind, block],
                recv_sem=cross.at[block],
                device_id=other,
                device_id_type=MESH,
            )
            pl.when(amount == chosen)(copy.wait_send)

    def all_sent(block):
        first = tall_first(block)
        across = jnp.where(first, 1, side)
        up = jnp.where(z + 1 < tall, (z + 1) * across, 0)
        down = jnp.where(z > 0, (tall - z) * across, 0)
        choices = sorted({n * m for n in range(1, tall + 1) for m in (1, side)})
        sent(0, block, up, choices)
        sent(1, block, down, choices)
        height = jnp.where(first, tall, 1)
        if side == 2:
            sent(2, block, height, (1, tall))
        else:
            choices = sorted({n * m for n in range(1, side + 1) for m in (1, tall)})
            sent(2, block, jnp.where(u + 1 < side, (u + 1) * height, 0), choices)
            sent(3, block, jnp.where(u > 0, (side - u) * height, 0), choices)
        plane = tall * side
        if side == 2:
            sent(4, block, jnp.int32(plane), (plane,))
        else:
            choices = [n * plane for n in range(1, side + 1)]
            sent(4, block, jnp.where(v + 1 < side, (v + 1) * plane, 0), choices)
            sent(5, block, jnp.where(v > 0, (side - v) * plane, 0), choices)
        hand_over(many(block, pieces), block).wait_send()

    def arrived(block, pz, pu, pv):
        link(0, block, number(pz, pu, pv), other).wait_recv()
        pass_on(block, pz, pu, pv)

    low = jnp.minimum(z, tall - 1 - z)

    def near(k):
        step = jnp.where(lax.rem(k, 2) == 1, low - lax.div(k + 1, 2), low + lax.div(k, 2))
        at = jnp.where(k <= 2 * low, step, k)
        return jnp.where(z == low, at, tall - 1 - at)

    def own_copies(block):
        rows = pl.ds(pl.multiple_of((here * 2 + core) * depth, depth), depth)
        first = pl.multiple_of(block * LANES, LANES)
        for half, source in enumerate((value_hbm, gate_hbm)):
            yield pltpu.make_async_copy(
                source.at[:, pl.ds(first, LANES)],
                weights.at[block, rows, pl.ds(half * LANES, LANES)],
                own.at[block, half],
            )

    def send_own(block):
        for copy in own_copies(block):
            copy.wait()
        pass_on(block, z, u, v)

    barrier = pltpu.get_barrier_semaphore()
    greeted = jnp.int32(1)
    pl.semaphore_signal(barrier, inc=1, device_id=other, device_id_type=MESH)
    for there, target in (
        (z + 1 < tall, device(z + 1, u, v)),
        (z > 0, device(z - 1, u, v)),
        (u + 1 < side, device(z, u + 1, v)),
        (u > 0, device(z, u - 1, v)),
        (v + 1 < side, device(z, u, v + 1)),
        (v > 0, device(z, u, v - 1)),
        (sp + 1 < sp_size, {"sp": sp + 1, "dp": dp}),
        (sp > 0, {"sp": sp - 1, "dp": dp}),
    ):
        greeted = greeted + there.astype(jnp.int32)

        @pl.when(there)
        def _(target=target):
            pl.semaphore_signal(barrier, inc=1, device_id=target, device_id_type=MESH)

    @pl.loop(0, blocks)
    def _(block):
        for copy in own_copies(block):
            copy.start()

    load = pltpu.make_async_copy(tok_hbm, tok, begin.at[0])
    load.start()
    read = pltpu.make_async_copy(docs_hbm, docs.at[:, pl.ds(LANES, count)], begin.at[1])
    read.start()
    small = [
        pltpu.make_async_copy(source, target, begin.at[2 + i])
        for i, (source, target) in enumerate(
            ((conv_hbm, conv_ref), (gain_hbm, gain_ref), (bias_hbm, bias_ref))
        )
    ]
    for copy in small:
        copy.start()

    pl.semaphore_wait(barrier, greeted)

    following = {"sp": lax.rem(sp + 1, sp_size), "dp": dp}
    def tail(block):
        return pltpu.make_async_remote_copy(
            src_ref=trailing.at[block],
            dst_ref=leading.at[block],
            send_sem=halo.at[0, block],
            recv_sem=halo.at[1, block],
            device_id=following,
            device_id_type=MESH,
        )

    docs_tail = pltpu.make_async_remote_copy(
        src_ref=docs_hbm.at[:, pl.ds(count - LANES, LANES)],
        dst_ref=docs.at[:, pl.ds(0, LANES)],
        send_sem=halo.at[0, blocks],
        recv_sem=halo.at[1, blocks],
        device_id=following,
        device_id_type=MESH,
    )

    @pl.when(sp + 1 < sp_size)
    def _():
        docs_tail.start()

    ahead = min(blocks, -(-order["own"] // tall))

    @pl.loop(0, ahead)
    def _(block):
        send_own(block)

    @pl.when(sp == 0)
    def _():
        leading[...] = jnp.zeros_like(leading)
        docs[:, pl.ds(0, LANES)] = jnp.full((1, LANES), -1, jnp.int32)

    def prepare():
        load.wait()
        read.wait()
        for copy in small:
            copy.wait()
        taps[pl.ds(0, KERNEL), :] = conv_ref[...].astype(jnp.float32)

        @pl.when(sp > 0)
        def _():
            docs_tail.wait_recv()

        column = jnp.broadcast_to(docs[...], (LANES, LANES + count)).T
        wide = column[LANES - HALO :]
        for lag in range(8, HALO, 8):
            same = wide[HALO - 8 :] == wide[HALO - 8 - lag : HALO + count - lag]
            far[lag // 8 - 1, pl.ds(HALO - 8, count + 8), :] = same.astype(jnp.float32)
        for lag in range(1, 8):
            same = wide[HALO:] == wide[HALO - lag : HALO + count - lag]
            near_by[lag - 1, pl.ds(0, count), :] = same.astype(jnp.float32)

        total[...] = jnp.zeros_like(total)
        square[...] = jnp.zeros_like(square)

    def project(block, half):
        rows = pl.ds(half * span, span)
        both = jnp.dot(tok[rows, :], weights[block], preferred_element_type=jnp.float32)
        value = both[:, :LANES].astype(jnp.bfloat16).astype(jnp.float32)
        gate = both[:, LANES:].astype(jnp.bfloat16).astype(jnp.float32)
        glu = (value * jax.nn.sigmoid(gate)).astype(jnp.bfloat16)
        base = lax.rem(block, slots) * (HALO // 8)
        shifted[base, pl.ds(HALO + half * span, span), :] = glu.astype(jnp.float32)
        if half:
            trailing[block] = glu[span - HALO :]

    def exchange(block):
        @pl.when(sp + 1 < sp_size)
        def _():
            tail(block).start()

    def convolve(block, half):
        lanes = pl.ds(pl.multiple_of(block * LANES, LANES), LANES)
        base = lax.rem(block, slots) * (HALO // 8)
        if half == 0:
            @pl.when(sp > 0)
            def _():
                tail(block).wait_recv()

            shifted[base, pl.ds(0, HALO), :] = leading[block].astype(jnp.float32)
        start = half * span + HALO - 8
        kept = pl.ds(start, span + 8)
        for a in range(1, HALO // 8):
            moved = shifted[base, pl.ds(start - 8 * a, span + 8), :]
            shifted[base + a, kept, :] = moved * far[a - 1, kept, :]

        @pl.loop(0, span // TILE)
        def _(tile):
            top = pl.multiple_of(half * span + tile * TILE, TILE)
            held = None
            for r in range(8):
                run = None
                for a in range(HALO // 8):
                    lag = 8 * a + r
                    if lag < KERNEL:
                        moved = shifted[base + a, pl.ds(top + HALO - r, TILE), :]
                        term = moved * taps[lag : lag + 1, lanes]
                        run = term if run is None else run + term
                if r:
                    run = run * near_by[r - 1, pl.ds(top, TILE), :]
                held = run if held is None else held + run
            rows = pl.ds(top, TILE)
            rounded = held.astype(jnp.bfloat16)
            mixed[rows, lanes] = rounded
            held = rounded.astype(jnp.float32)

            @pl.when(block == 0)
            def _():
                middle = jnp.mean(held, axis=-1, keepdims=True)
                center[rows, :] = jnp.broadcast_to(middle, (TILE, LANES))

            off = held - center[rows, :]
            total[rows, :] += off
            square[rows, :] += off * off

    def finish():
        moved = jnp.sum(total[...], axis=-1, keepdims=True) / channels
        spread = jnp.sum(square[...], axis=-1, keepdims=True) / channels - moved * moved
        scale = lax.rsqrt(jnp.maximum(spread, 0.0) + 1e-06)
        center[...] = center[...] + moved
        total[...] = jnp.broadcast_to(scale, total.shape)

        @pl.loop(0, count // LEAVE)
        def _(step):
            rows = pl.ds(pl.multiple_of(step * LEAVE, LEAVE), LEAVE)
            middle, scale = center[rows, :], total[rows, :]
            for lane in range(0, channels, LANES):
                lanes = pl.ds(lane, LANES)
                wide = mixed[rows, lanes].astype(jnp.float32)
                normed = (wide - middle) * scale * gain_ref[:, lanes] + bias_ref[:, lanes]
                mixed[rows, lanes] = (normed * jax.nn.sigmoid(normed)).astype(jnp.bfloat16)

    def level(k):
        return z if k == 0 else near(k)

    def near_u(block, k):
        @pl.loop(1, side)
        def _(du):
            arrived(block, level(k), lax.rem(u + du, side), v)

    def near_v(block, k):
        @pl.loop(1, side)
        def _(dv):
            arrived(block, level(k), u, lax.rem(v + dv, side))

    def far_v(block, k):
        @pl.loop(1, side)
        def _(du):
            @pl.loop(1, side)
            def _(dv):
                arrived(block, level(k), lax.rem(u + du, side), lax.rem(v + dv, side))

    def compute(block, k):
        if k == 0:
            pl.when(block == 0)(prepare)
            hand_over(many(block, pieces), block).wait_recv()

            project(block, 1)
        if k == 1:
            exchange(block)
            project(block, 0)
        if k == tall - 1:
            all_sent(block)

    sites = [(-order["own"], lambda block: send_own(block))]
    for k in range(1, tall):
        sites.append((order["along_z"][k - 1], lambda block, k=k: arrived(block, near(k), u, v)))
    for name, act in (("along_u", near_u), ("near_v", near_v), ("far_v", far_v)):
        for k in range(tall):
            sites.append((order[name][k], lambda block, k=k, act=act: act(block, k)))
    assert all(offset <= order["late"] for offset, _ in sites)
    for k in range(tall):
        sites.append((order["late"] + k, lambda block, k=k: compute(block, k)))
    for half in range(2):
        place = order["late"] + (2 if half else order["after"] + 1)
        sites.append((place, lambda block, half=half: convolve(block, half)))

    def round_of(number, carry):
        for j in range(tall):
            for offset, act in sites:
                if offset % tall != j:
                    continue
                block = number - offset // tall
                first = ahead if offset < 0 else 0

                @pl.when((block >= first) & (block < blocks))
                def _(block=block, act=act):
                    act(block)

        return carry

    rounds = blocks + (order["late"] + order["after"] + tall) // tall
    lax.fori_loop(0, rounds, round_of, 0)
    finish()

    @pl.when(sp + 1 < sp_size)
    def _():
        @pl.loop(0, blocks)
        def _(block):
            tail(block).wait_send()

        docs_tail.wait_send()


def activated_product(
    rows, docs, value_weight, gate_weight, conv_weight, norm_gain, norm_bias
):
    side = lax.axis_size("dp") // 2
    tall = lax.axis_size("sp") // side
    count, width = rows.shape
    channels = value_weight.shape[1]
    order = plan(side, tall, channels)
    blocks = order["blocks"]
    slots = (order["after"] + 1) // tall + 1
    pieces = tall * side * side
    return pl.pallas_call(
        functools.partial(fused_kernel, side, tall, order),
        out_shape=pltpu.VMEM((count, channels), jnp.bfloat16),
        in_specs=[pl.BlockSpec(memory_space=pl.ANY)] * 7,
        out_specs=pl.BlockSpec(memory_space=pltpu.VMEM),
        scratch_shapes=[
            pltpu.VMEM((blocks, width, 2 * channels // blocks), jnp.bfloat16),
            pltpu.VMEM((count, width), jnp.bfloat16),
            pltpu.VMEM((1, LANES + count), jnp.int32),
            pltpu.VMEM(conv_weight.shape, conv_weight.dtype),
            pltpu.VMEM((1, channels), jnp.float32),
            pltpu.VMEM((1, channels), jnp.float32),
            pltpu.VMEM((blocks, HALO, LANES), jnp.bfloat16),
            pltpu.VMEM((blocks, HALO, LANES), jnp.bfloat16),
            pltpu.VMEM((HALO, channels), jnp.float32),
            pltpu.VMEM((slots * (HALO // 8), HALO + count + SPARE, LANES), jnp.float32),
            pltpu.VMEM((HALO // 8 - 1, HALO + count + SPARE, LANES), jnp.float32),
            pltpu.VMEM((7, count + SPARE, LANES), jnp.float32),
            pltpu.VMEM((count, LANES), jnp.float32),
            pltpu.VMEM((count, LANES), jnp.float32),
            pltpu.VMEM((count, LANES), jnp.float32),
            pltpu.SemaphoreType.DMA((7, blocks)),
            pltpu.SemaphoreType.DMA((blocks, pieces)),
            pltpu.SemaphoreType.DMA((blocks,)),
            pltpu.SemaphoreType.DMA((blocks, 2)),
            pltpu.SemaphoreType.DMA((5,)),
            pltpu.SemaphoreType.DMA((2, blocks + 1)),
        ],
        compiler_params=pltpu.CompilerParams(
            collective_id=0, has_side_effects=True, vmem_limit_bytes=56 * 1024 * 1024
        ),
    )(
        rows, docs, value_weight, gate_weight, conv_weight, norm_gain[None], norm_bias[None]
    )


def per_device(tokens, documents, value_weight, gate_weight, conv_weight, norm_gain, norm_bias):
    batch, count, width = tokens.shape
    channels = value_weight.shape[1]
    rows = tokens.reshape(batch * count, width)
    out = activated_product(
        rows, documents, value_weight, gate_weight, conv_weight, norm_gain, norm_bias
    )
    return out.reshape(batch, count, channels)


def solution(mesh):
    return jax.shard_map(
        per_device,
        mesh=mesh,
        in_specs=(
            P("dp", "sp", None),
            P("dp", "sp"),
            P(("sp", "dp"), None),
            P(("sp", "dp"), None),
            P(),
            P(),
            P(),
        ),
        out_specs=P("dp", "sp", None),
        check_vma=False,
    )
```
